256 devices in a mesh: sp: 64 (over z, x, core), tp: 4 (over y).
Axes of the slice: x: 4, y: 4, z: 8, core: 2. Of those that a mesh axis runs over, the one named last changes fastest.
Arguments:
- query_wide: bfloat16 [8192, 1536], P('sp', 'tp'), may hold values from -600 to 600
- query_narrow: bfloat16 [8192, 1024], P('sp', 'tp'), may hold values from -600 to 600
- latent: bfloat16 [8192, 512], P('sp'), may hold values from -6 to 6
- rope_key: bfloat16 [8192, 64], P('sp'), may hold values from -6 to 6
- latent_norm_weight: float32 [512], replicated, may hold values from 0.1 to 1.9
- broad_key_lift: bfloat16 [512, 1024], P(None, 'tp'), may hold values from -0.25 to 0.25
- broad_value_lift: bfloat16 [512, 1024], P(None, 'tp'), may hold values from -0.25 to 0.25
- slim_key_lift: bfloat16 [512, 512], P(None, 'tp'), may hold values from -0.25 to 0.25
- slim_value_lift: bfloat16 [512, 512], P(None, 'tp'), may hold values from -0.25 to 0.25
- out_wide: bfloat16 [1024, 2048], P('tp'), may hold values from -0.4375 to 0.4375
- out_narrow: bfloat16 [512, 2048], P('tp'), may hold values from -0.4375 to 0.4375
- resid: bfloat16 [8192, 2048], P('sp'), may hold values from -20 to 20
- ffn_gain: float32 [2048], replicated, may hold values from 0.1 to 1.9
- group_route: int32 [8192], P('sp'), may hold values from 0 to 63, as said below
- expert_pair: int32 [8192, 2], P('sp'), may hold values from 0 to 3, all different within a row
- group_prob: float32 [8192], P('sp'), may hold values from 0.2 to 1
- expert_prob: float32 [8192, 2], P('sp'), may hold values from 0.05 to 1
- gate_weight: bfloat16 [64, 4, 2048, 512], P('sp', None, None, 'tp'), may hold values from -0.125 to 0.125
- up_weight: bfloat16 [64, 4, 2048, 512], P('sp', None, None, 'tp'), may hold values from -0.125 to 0.125
- down_weight: bfloat16 [64, 4, 512, 2048], P('sp', None, 'tp'), may hold values from -0.25 to 0.25
Outputs:
- mixed: bfloat16 [8192, 2048], P('sp', 'tp')
The draws below stay inside these ranges and needn't reach their ends.
Inputs may be any that keep to these rules, and one draw needn't show every extreme that they name: `group_route`: of the 128 tokens of one index of sp at most 4 name one group; in every draw one group is named by exactly 4 tokens of every index of sp, and every index of sp names one more group exactly 4 times. `expert_pair`: A token's two experts are different.
All inputs are finite; a program needn't handle non-finite values.
Results may differ from the reference program's by a relative error of at most 0.017.
Values may be sent and summed in bfloat16 or wider, within the bound.
A program may use at most 128 MiB of HBM per device.

```python
import math
import jax
import jax.numpy as jnp
from jax import lax

D = 2048
WIDE_HEADS = 8
SLIM_HEADS = 8
PLAIN_WIDTH_WIDE = 128
PLAIN_WIDTH_SLIM = 64
ROPE = 64
VALUE_WIDTH_WIDE = 128
VALUE_WIDTH_SLIM = 64
LATENT_RANK = 512
EPG = 4
FF = 512
TOK_DEV = 128
TOKEN_COUNT = 8192
GROUPS = 64
CAP = 4
N_SP = 64
N_TP = 4


def query_draw(key, columns):
    base_values = 2.5 * jax.random.truncated_normal(key, -6.0, 6.0, (TOKEN_COUNT, columns), jnp.float32)
    return base_values.astype(jnp.bfloat16)


def draw_query_wide(key, part):
    return query_draw(jax.random.fold_in(key, 3), WIDE_HEADS * (PLAIN_WIDTH_WIDE + ROPE))


def draw_query_narrow(key, part):
    return query_draw(jax.random.fold_in(key, 5), SLIM_HEADS * (PLAIN_WIDTH_SLIM + ROPE))


def draw_resid(key, part):
    column = jnp.arange(D).astype(jnp.float32)
    column_scale = 0.3 * 9.0 ** (column / (D - 1))
    base_values = jax.random.truncated_normal(jax.random.fold_in(key, 19), -6.0, 6.0, (TOKEN_COUNT, D), jnp.float32)
    return (base_values * column_scale[None, :]).astype(jnp.bfloat16)


def draw_group_route(key, part):
    heavy_all = jax.random.randint(jax.random.fold_in(key, 11), (), 0, GROUPS)
    slot_group = (jnp.arange(GROUPS * CAP) // CAP).astype(jnp.int32)

    def one_device(device_index):
        device_key = jax.random.fold_in(jax.random.fold_in(key, 13), device_index)
        first_key, second_key, third_key = jax.random.split(device_key, 3)
        second_group = (heavy_all + 1 + jax.random.randint(first_key, (), 0, GROUPS - 1)) % GROUPS
        shuffled = jax.random.permutation(second_key, GROUPS * CAP)
        position = jnp.zeros((GROUPS * CAP,), jnp.int32).at[shuffled].set(jnp.arange(GROUPS * CAP, dtype=jnp.int32))
        heavy_slot = (slot_group == heavy_all) | (slot_group == second_group)
        sort_score = jnp.where(heavy_slot, jnp.arange(GROUPS * CAP, dtype=jnp.int32), GROUPS * CAP + position)
        picked = slot_group[jnp.argsort(sort_score, stable=True)][:TOK_DEV]
        return picked[jax.random.permutation(third_key, TOK_DEV)]
    return jax.vmap(one_device)(jnp.arange(GROUPS)).reshape(TOKEN_COUNT).astype(jnp.int32)


def level_of(own_key, dims, cuts, low, high):
    gain = 1.0
    for axis_at, blocks in cuts:
        steps = jax.random.uniform(jax.random.fold_in(jax.random.fold_in(own_key, 6), axis_at), (blocks,), jnp.float32, low / len(cuts), high / len(cuts))
        gain = gain * jnp.repeat(jnp.exp(steps), dims[axis_at] // blocks).reshape((-1,) + (1,) * (len(dims) - 1 - axis_at))
    return gain


def choose_distinct(own_key, rows, number_of, top, lift):
    sequence = jax.random.permutation(jax.random.fold_in(own_key, 1), number_of)
    favour = sequence
    for power in range(3):
        favour = favour * favour // number_of
    favour = favour * lift // number_of
    lots = jax.random.randint(jax.random.fold_in(own_key, 2), (rows, number_of), 0, 4096) + favour
    holders = jax.random.permutation(jax.random.fold_in(own_key, 3), rows)[jnp.arange(number_of) % rows]
    lots = jnp.where(jnp.arange(rows)[:, None] == holders[None, :], 1 << 14, lots)
    priority = lots * number_of + jnp.arange(number_of)
    return lax.top_k(priority.astype(jnp.int32), top)[1].astype(jnp.int32)


def noise(rng, extent, scale, bound, pieces=(), held_as=jnp.bfloat16):
    factor_of = level_of(rng, extent, pieces, -0.22, 0.18) if pieces else 1.0
    result = jax.random.normal(rng, extent, jnp.float32) * scale * factor_of
    return jnp.minimum(jnp.maximum(result, -bound), bound).astype(held_as)


def setup_inputs(seed: int = 0) -> dict:
    seeds = jax.random.split(jax.random.key(seed), 21)
    return {
        "query_wide": draw_query_wide(jax.random.fold_in(seeds[20], 71), 0),
        "query_narrow": draw_query_narrow(jax.random.fold_in(seeds[20], 71), 0),
        "latent": noise(seeds[2], (TOKEN_COUNT, LATENT_RANK), 1.0, 6.0, ((0, 64),)),
        "rope_key": noise(seeds[3], (TOKEN_COUNT, ROPE), 1.0, 6.0, ((0, 64),)),
        "latent_norm_weight": jnp.clip(1.0 + 0.18 * jax.random.normal(seeds[4], (LATENT_RANK,), jnp.float32), 0.1, 1.9),
        "broad_key_lift": noise(seeds[5], (LATENT_RANK, WIDE_HEADS * PLAIN_WIDTH_WIDE), LATENT_RANK ** -0.5, 0.25, ((1, 4),)),
        "broad_value_lift": noise(seeds[6], (LATENT_RANK, WIDE_HEADS * VALUE_WIDTH_WIDE), LATENT_RANK ** -0.5, 0.25, ((1, 4),)),
        "slim_key_lift": noise(seeds[7], (LATENT_RANK, SLIM_HEADS * PLAIN_WIDTH_SLIM), LATENT_RANK ** -0.5, 0.25, ((1, 4),)),
        "slim_value_lift": noise(seeds[8], (LATENT_RANK, SLIM_HEADS * VALUE_WIDTH_SLIM), LATENT_RANK ** -0.5, 0.25, ((1, 4),)),
        "out_wide": noise(seeds[9], (WIDE_HEADS * VALUE_WIDTH_WIDE, D), ((WIDE_HEADS * VALUE_WIDTH_WIDE + SLIM_HEADS * VALUE_WIDTH_SLIM) // 9) ** -0.5, 0.4375, ((0, 4),)),
        "out_narrow": noise(seeds[10], (SLIM_HEADS * VALUE_WIDTH_SLIM, D), ((WIDE_HEADS * VALUE_WIDTH_WIDE + SLIM_HEADS * VALUE_WIDTH_SLIM) // 9) ** -0.5, 0.4375, ((0, 4),)),
        "resid": draw_resid(jax.random.fold_in(seeds[20], 71), 0),
        "ffn_gain": jnp.clip(1.0 + 0.18 * jax.random.normal(seeds[12], (D,), jnp.float32), 0.1, 1.9),
        "group_route": draw_group_route(jax.random.fold_in(seeds[20], 71), 0),
        "expert_pair": choose_distinct(seeds[14], TOKEN_COUNT, EPG, 2, 0),
        "group_prob": jnp.clip(0.2 + 0.8 * jax.random.uniform(seeds[15], (TOKEN_COUNT,), jnp.float32) ** level_of(seeds[15], (TOKEN_COUNT,), ((0, 64),), -0.2, 0.2), 0.2, 1.0),
        "expert_prob": jnp.clip(jnp.exp(math.log(1.0) - 2.9957323 * jax.random.uniform(seeds[16], (TOKEN_COUNT, 2), jnp.float32) ** level_of(seeds[16], (TOKEN_COUNT, 2), ((0, 64),), -0.2, 0.2)), 0.05, 1.0),
        "gate_weight": noise(seeds[17], (GROUPS, EPG, D, FF), D ** -0.5, 0.125, ((0, 64), (3, 4))),
        "up_weight": noise(seeds[18], (GROUPS, EPG, D, FF), D ** -0.5, 0.125, ((0, 64), (3, 4))),
        "down_weight": noise(seeds[19], (GROUPS, EPG, FF, D), FF ** -0.5, 0.25, ((0, 64), (2, 4))),
    }


ROPE_BASE = 10000.0
EPSILON = 1e-06

def rms_scale(values, gain_row):
    widened = values.astype(jnp.float32)
    return widened * lax.rsqrt(lax.optimization_barrier(jnp.mean(widened * widened, axis=-1, keepdims=True)) + EPSILON) * gain_row.astype(jnp.float32)

def angles(positions, width):
    frequency = 1.0 / ROPE_BASE ** (jnp.arange(0, width, 2).astype(jnp.float32) / width)
    return positions.astype(jnp.float32)[:, None] * frequency[None, :]

def rotary(values, angle_table):
    half_width = values.shape[-1] // 2
    first_half = values[..., :half_width]
    second = values[..., half_width:]
    return jnp.concatenate([first_half * jnp.cos(angle_table) - second * jnp.sin(angle_table), second * jnp.cos(angle_table) + first_half * jnp.sin(angle_table)], axis=-1)

def stored(values):
    return lax.optimization_barrier(values.astype(jnp.bfloat16)).astype(jnp.float32)

def attention(query_nope, query_rot, key_nope, key_rot, value_rows, scale):
    key_pos = jnp.arange(TOKEN_COUNT).astype(jnp.int32)

    def one_block(block_index):
        first_row = (block_index * TOK_DEV).astype(jnp.int32)
        nope_rows = lax.dynamic_slice_in_dim(query_nope, first_row, TOK_DEV, 0)
        rot_rows = lax.dynamic_slice_in_dim(query_rot, first_row, TOK_DEV, 0)
        scores = jnp.einsum('thd,khd->htk', nope_rows, key_nope) + jnp.einsum('thd,kd->htk', rot_rows, key_rot)
        scores = scores * scale
        query_pos = first_row + jnp.arange(TOK_DEV).astype(jnp.int32)
        scores = jnp.where((query_pos[:, None] >= key_pos[None, :])[None], scores, -jnp.inf)
        row_peak = lax.optimization_barrier(jnp.max(scores, axis=-1, keepdims=True))
        weights = jnp.exp(scores - row_peak)
        row_total = lax.optimization_barrier(jnp.sum(weights, axis=-1))
        mixed_rows = jnp.einsum('htk,khd->thd', stored(weights), value_rows)
        return (mixed_rows / row_total.T[:, :, None]).astype(jnp.bfloat16)
    blocks = lax.map(one_block, jnp.arange(TOKEN_COUNT // TOK_DEV).astype(jnp.int32))
    return blocks.reshape(TOKEN_COUNT, -1)

def reference(query_wide, query_narrow, latent, rope_key, latent_norm_weight, broad_key_lift, broad_value_lift, slim_key_lift, slim_value_lift, out_wide, out_narrow, resid, ffn_gain, group_route, expert_pair, group_prob, expert_prob, gate_weight, up_weight, down_weight):
    angle_table = angles(jnp.arange(TOKEN_COUNT).astype(jnp.int32), ROPE)
    latent_rows = rms_scale(latent, latent_norm_weight).astype(jnp.bfloat16)
    key_rot = stored(rotary(rope_key.astype(jnp.float32), angle_table))
    key_wide = stored(jnp.dot(latent_rows, broad_key_lift, preferred_element_type=jnp.float32)).reshape(TOKEN_COUNT, WIDE_HEADS, PLAIN_WIDTH_WIDE)
    value_wide = stored(jnp.dot(latent_rows, broad_value_lift, preferred_element_type=jnp.float32)).reshape(TOKEN_COUNT, WIDE_HEADS, VALUE_WIDTH_WIDE)
    key_narrow = stored(jnp.dot(latent_rows, slim_key_lift, preferred_element_type=jnp.float32)).reshape(TOKEN_COUNT, SLIM_HEADS, PLAIN_WIDTH_SLIM)
    value_narrow = stored(jnp.dot(latent_rows, slim_value_lift, preferred_element_type=jnp.float32)).reshape(TOKEN_COUNT, SLIM_HEADS, VALUE_WIDTH_SLIM)
    wide_rows = query_wide.reshape(TOKEN_COUNT, WIDE_HEADS, PLAIN_WIDTH_WIDE + ROPE).astype(jnp.float32)
    wide_rot = stored(rotary(wide_rows[..., PLAIN_WIDTH_WIDE:], angle_table[:, None, :]))
    narrow_rows = query_narrow.reshape(TOKEN_COUNT, SLIM_HEADS, PLAIN_WIDTH_SLIM + ROPE).astype(jnp.float32)
    narrow_rot = stored(rotary(narrow_rows[..., PLAIN_WIDTH_SLIM:], angle_table[:, None, :]))
    att_wide = attention(wide_rows[..., :PLAIN_WIDTH_WIDE], wide_rot, key_wide, key_rot, value_wide, (PLAIN_WIDTH_WIDE + ROPE) ** (-0.5))
    att_narrow = attention(narrow_rows[..., :PLAIN_WIDTH_SLIM], narrow_rot, key_narrow, key_rot, value_narrow, (PLAIN_WIDTH_SLIM + ROPE) ** (-0.5))
    wide_share = WIDE_HEADS // N_TP * VALUE_WIDTH_WIDE
    narrow_share = SLIM_HEADS // N_TP * VALUE_WIDTH_SLIM
    projected = jnp.zeros((TOKEN_COUNT, D), jnp.float32)
    for part_index in range(N_TP):
        wide_lo = part_index * wide_share
        narrow_lo = part_index * narrow_share
        partial_value = jnp.dot(att_wide[:, wide_lo:wide_lo + wide_share], out_wide[wide_lo:wide_lo + wide_share], preferred_element_type=jnp.float32)
        partial_value = partial_value + jnp.dot(att_narrow[:, narrow_lo:narrow_lo + narrow_share], out_narrow[narrow_lo:narrow_lo + narrow_share], preferred_element_type=jnp.float32)
        projected = projected + stored(partial_value)
    stream = (resid.astype(jnp.float32) + projected).astype(jnp.bfloat16)
    normed = rms_scale(stream, ffn_gain).astype(jnp.bfloat16)
    share_of = group_prob[:, None] * expert_prob / lax.optimization_barrier(jnp.sum(expert_prob, axis=1, keepdims=True))
    chosen = (expert_pair[:, :, None] == jnp.arange(EPG).astype(jnp.int32)[None, None, :]).astype(jnp.float32)
    combine = lax.optimization_barrier(jnp.sum(share_of[:, :, None] * chosen, axis=1)).astype(jnp.bfloat16)
    slot_count = N_SP * CAP
    member = (group_route[:, None] == jnp.arange(GROUPS).astype(jnp.int32)[None, :]).astype(jnp.int32)
    group_rank = lax.optimization_barrier(jnp.sum(jnp.cumsum(member, axis=0) * member, axis=1)) - 1
    slot_index = (group_route * slot_count + group_rank).astype(jnp.int32)
    routed_rows = jnp.zeros((GROUPS * slot_count, D), jnp.bfloat16).at[slot_index].set(normed)
    routed_weights = jnp.zeros((GROUPS * slot_count, EPG), jnp.bfloat16).at[slot_index].set(combine)

    def one_group(operands):
        group_rows, group_weights, gate_group, up_group, down_group = operands
        flat_rows = stored(group_rows)
        gate_act = jnp.einsum('rd,edf->ref', flat_rows, gate_group.astype(jnp.float32))
        up_act = jnp.einsum('rd,edf->ref', flat_rows, up_group.astype(jnp.float32))
        hidden = stored(jax.nn.silu(gate_act) * up_act * group_weights.astype(jnp.float32)[:, :, None])
        hidden = hidden.reshape(slot_count, EPG, N_TP, FF // N_TP)
        down_split = down_group.astype(jnp.float32).reshape(EPG, N_TP, FF // N_TP, D)
        partials = stored(jnp.einsum('repf,epfd->prd', hidden, down_split))
        return lax.optimization_barrier(jnp.sum(partials, axis=0)).astype(jnp.bfloat16)
    results = lax.map(one_group, (routed_rows.reshape(GROUPS, slot_count, D), routed_weights.reshape(GROUPS, slot_count, EPG), gate_weight, up_weight, down_weight))
    moe = results.reshape(GROUPS * slot_count, D)[slot_index]
    return (stream.astype(jnp.float32) + moe.astype(jnp.float32)).astype(jnp.bfloat16)
```

```python
import functools

import jax
import jax.numpy as jnp
from jax import lax
from jax.experimental import pallas as pl
from jax.experimental.pallas import tpu as pltpu
from jax.sharding import PartitionSpec as P

PLAIN_WIDTH_WIDE = 128
PLAIN_WIDTH_SLIM = 64
ROPE = 64
VALUE_WIDTH_WIDE = 128
VALUE_WIDTH_SLIM = 64
EPG = 4


ROPE_BASE = 10000.0
EPSILON = 1e-06
MASKED = -1e30


def in_blocks(x, dim, peers):
    before, after = (x.shape[:dim], x.shape[dim + 1 :])
    return jnp.moveaxis(x.reshape(*before, peers, -1, *after), dim, 0)


def sum_at_owner(x, axis, dim):
    blocks = in_blocks(x, dim, lax.axis_size(axis))
    arrived = lax.all_to_all(blocks, axis, split_axis=0, concat_axis=0, tiled=True)
    return arrived.astype(jnp.float32).sum(axis=0)


def sent_to_all(x, axis):
    copies = jnp.broadcast_to(x, (lax.axis_size(axis), *x.shape))
    return lax.all_to_all(copies, axis, split_axis=0, concat_axis=0, tiled=True)


def of_everyone(x, axis):
    everything = sent_to_all(x, axis)
    return jnp.sum(everything, axis=0)


def joined_along(blocks, dim):
    blocks = jnp.moveaxis(blocks, 0, dim)
    shape = blocks.shape
    return blocks.reshape(*shape[:dim], shape[dim] * shape[dim + 1], *shape[dim + 2 :])


def gathered_copies(x, axis, dim):
    blocks = sent_to_all(x, axis)
    return joined_along(blocks, dim)


def rms_scale(values, gain_row):
    widened = values.astype(jnp.float32)
    return (
        widened
        * lax.rsqrt(jnp.mean(widened * widened, axis=-1, keepdims=True) + EPSILON)
        * gain_row
    )


def angles(positions, width):
    frequency = 1.0 / ROPE_BASE ** (jnp.arange(0, width, 2).astype(jnp.float32) / width)
    return positions.astype(jnp.float32)[:, None] * frequency[None, :]


MESH = pl.DeviceIdType.MESH
LOG2E = 1.4426950408889634
Z = 8
XC = 8
BLOCK = 128
HEAD_ROWS = ((0, 128), (128, 256), (256, 320), (320, 384))
HEAD_QUERY = ((0, 256), (128, 384), (384, 512), (512, 640))
HEAD_KEY = ((0, 256), (256, 512), (512, 640), (640, 768))
HEAD_SCALE = (192**-0.5 * LOG2E, 192**-0.5 * LOG2E, 128**-0.5 * LOG2E, 128**-0.5 * LOG2E)


def nt(a, b):
    return lax.dot_general(a, b, (((1,), (1,)), ((), ())), preferred_element_type=jnp.float32)


def nn(a, b):
    return lax.dot_general(a, b, (((1,), (0,)), ((), ())), preferred_element_type=jnp.float32)


def remote(src, dst, send_sem, recv_sem, sp):
    return pltpu.make_async_remote_copy(
        src_ref=src,
        dst_ref=dst,
        send_sem=send_sem,
        recv_sem=recv_sem,
        device_id={"sp": sp},
        device_id_type=MESH,
    )


def attention_kernel(
    qw_ref, qn_ref, latent_ref, rope_ref, gain_ref, wbk_ref, wbv_ref, wsk_ref, wsv_ref, cos_ref, sin_ref,
    out_ref,
    q_all, lat_all, keys, values, acc, peak, total, o_send, o_recv, s_send, s_recv,
    q_ssem, q_rsem, up_ssem, up_rsem, dn_ssem, dn_rsem, o_ssem, o_rsem, t_ssem, t_rsem,
):
    sp = lax.axis_index("sp")
    z = sp // XC
    xc = lax.rem(sp, XC)
    core = lax.rem(xc, 2)
    base = z * XC
    sibling = base + xc + 1 - 2 * core
    above = lax.rem(sp + XC, Z * XC)
    below = lax.rem(sp + (Z - 1) * XC, Z * XC)

    barrier = pltpu.get_barrier_semaphore()
    for d in range(1, XC):
        pl.semaphore_signal(barrier, inc=1, device_id={"sp": base + lax.rem(xc + d, XC)}, device_id_type=MESH)
    for peer in (above, below):
        pl.semaphore_signal(barrier, inc=1, device_id={"sp": peer}, device_id_type=MESH)

    lane = lax.broadcasted_iota(jnp.int32, (BLOCK, 128), 1)
    low = lane < 64
    first = lax.rem(lane, 64) < 32
    cos = cos_ref[...]
    sin = sin_ref[...]

    def turned(x):
        swapped = jnp.where(first, pltpu.roll(x, 96, 1), pltpu.roll(x, 32, 1))
        return x * cos + swapped * sin

    q_all[xc, :, 0:128] = qw_ref[:, 0:128]
    middle = qw_ref[:, 128:256].astype(jnp.float32)
    last = qw_ref[:, 256:384].astype(jnp.float32)
    q_all[xc, :, 128:256] = turned(jnp.where(low, middle, last)).astype(jnp.bfloat16)
    q_all[xc, :, 256:384] = pltpu.roll(jnp.where(low, last, middle), 64, 1).astype(jnp.bfloat16)
    for k in range(2):
        x = qn_ref[:, k * 128 : (k + 1) * 128].astype(jnp.float32)
        q_all[xc, :, 384 + k * 128 : 512 + k * 128] = jnp.where(low, x, turned(x)).astype(jnp.bfloat16)
    x = latent_ref[...].astype(jnp.float32)
    x = x * lax.rsqrt(jnp.mean(x * x, axis=1, keepdims=True) + EPSILON) * gain_ref[...]
    lat_all[z, :, 0:512] = x.astype(jnp.bfloat16)
    lat_all[z, :, 512:640] = turned(rope_ref[...].astype(jnp.float32)).astype(jnp.bfloat16)

    pl.semaphore_wait(barrier, XC + 1)

    def q_direct(d):
        return remote(
            q_all.at[xc], q_all.at[xc], q_ssem.at[d], q_rsem.at[d], base + lax.rem(xc + 2 * d, XC)
        )

    def q_sibling():
        return remote(q_all.at[xc], q_all.at[xc], q_ssem.at[0], q_rsem.at[0], sibling)

    def q_forward(d):
        slot = lax.rem(xc + 2 * (4 - d), XC)
        return remote(q_all.at[slot], q_all.at[slot], q_ssem.at[3 + d], q_rsem.at[3 + d], sibling)

    def up_copy(s):
        slot = lax.rem(z - s + 1 + Z, Z)
        return remote(lat_all.at[slot], lat_all.at[slot], up_ssem.at[s], up_rsem.at[s], above)

    def dn_copy(s):
        slot = lax.rem(z + s - 1, Z)
        return remote(lat_all.at[slot], lat_all.at[slot], dn_ssem.at[s], dn_rsem.at[s], below)

    def up_sends(s):
        return (s <= 4) & (z - s + 1 >= 0) & (z < Z - 1)

    def up_comes(s):
        return z - s >= 0

    def dn_sends(s):
        return (s <= 3) & (lax.rem(z + s - 1, Z) <= 2)

    def dn_comes(s):
        return (s <= 3) & (lax.rem(z + s, Z) <= 2)

    def start_step(s):
        @pl.when(up_sends(s))
        def _():
            up_copy(s).start()

        @pl.when(dn_sends(s))
        def _():
            dn_copy(s).start()

    def arrive_step(s):
        @pl.when(up_comes(s))
        def _():
            up_copy(s).wait_recv()

        @pl.when(dn_comes(s))
        def _():
            dn_copy(s).wait_recv()

    start_step(1)
    q_sibling().start()
    for d in range(1, 4):
        q_direct(d).start()

    peak[...] = jnp.full(peak.shape, MASKED, jnp.float32)
    total[...] = jnp.zeros(total.shape, jnp.float32)
    acc[...] = jnp.zeros(acc.shape, jnp.float32)

    def project(slot):
        rows = lat_all[slot, :, 0:512]
        rot = lat_all[slot, :, 512:640]
        wide = nn(rows, wbk_ref[...]).astype(jnp.bfloat16)
        zero = jnp.zeros_like(rot)
        keys[:, 0:128] = wide[:, 0:128]
        keys[:, 128:256] = jnp.where(low, rot, zero)
        keys[:, 256:384] = jnp.where(low, zero, rot)
        keys[:, 384:512] = wide[:, 128:256]
        slim = nn(rows, wsk_ref[...])
        keys[:, 512:640] = jnp.where(low, slim.astype(jnp.bfloat16), rot)
        keys[:, 640:768] = jnp.where(low, pltpu.roll(slim, 64, 1).astype(jnp.bfloat16), rot)
        values[0:256, :] = jnp.transpose(nn(rows, wbv_ref[...])).astype(jnp.bfloat16)
        values[256:384, :] = jnp.transpose(nn(rows, wsv_ref[...])).astype(jnp.bfloat16)

    def attend(slot, own):
        project(slot)

        def chunk(c, carry):
            if own:
                key_pos = xc * BLOCK + lax.broadcasted_iota(jnp.int32, (BLOCK, 256), 0)
                query_pos = c * 256 + lax.broadcasted_iota(jnp.int32, (BLOCK, 256), 1)
                seen = key_pos <= query_pos
            for h in range(4):
                ql, qh = HEAD_QUERY[h]
                kl, kh = HEAD_KEY[h]
                lo, hi = HEAD_ROWS[h]
                q = q_all[pl.ds(2 * c, 2), :, ql:qh].reshape(256, qh - ql)
                scores = nt(keys[:, kl:kh], q) * HEAD_SCALE[h]
                if own:
                    scores = jnp.where(seen, scores, MASKED)
                before = peak[c, h : h + 1, :]
                top = jnp.maximum(before, jnp.max(scores, axis=0, keepdims=True))
                keep = jnp.exp2(before - top)
                weights = jnp.exp2(scores - top)
                peak[c, h : h + 1, :] = top
                total[c, h : h + 1, :] = total[c, h : h + 1, :] * keep + jnp.sum(weights, axis=0, keepdims=True)
                acc[c, lo:hi, :] = acc[c, lo:hi, :] * keep + nn(values[lo:hi, :], weights.astype(jnp.bfloat16))
            return carry

        lax.fori_loop(0, 4, chunk, 0)

    arrive_step(1)
    start_step(2)
    for d in range(1, 4):
        q_direct(d).wait_recv()
        q_forward(d).start()
    q_sibling().wait_recv()
    for d in range(1, 4):
        q_forward(d).wait_recv()
    attend(z, True)

    def step(s, carry):
        @pl.when(s > 1)
        def _():
            arrive_step(s)
            start_step(s + 1)

        @pl.when(z - s >= 0)
        def _():
            attend(z - s, False)

        @pl.when((s <= 3) & (z + s >= Z))
        def _():
            attend(z + s - Z, False)

        return carry

    lax.fori_loop(1, 5, step, 0)

    for j in range(XC):
        c, lanes = j // 2, slice((j % 2) * 128, (j % 2) * 128 + 128)
        for h in range(4):
            lo, hi = HEAD_ROWS[h]
            o_send[j, lo:hi, :] = (acc[c, lo:hi, lanes] / total[c, h : h + 1, lanes]).astype(jnp.bfloat16)
            s_send[j, h : h + 1, :] = peak[c, h : h + 1, lanes]
            s_send[j, 4 + h : 5 + h, :] = total[c, h : h + 1, lanes]

    def o_copy(d):
        j = lax.rem(xc + d, XC)
        return remote(o_send.at[j], o_recv.at[xc], o_ssem.at[d], o_rsem.at[d], base + j)

    def s_copy(d):
        j = lax.rem(xc + d, XC)
        return remote(s_send.at[j], s_recv.at[xc], t_ssem.at[d], t_rsem.at[d], base + j)

    for d in range(1, XC):
        s_copy(d).start()
        o_copy(d).start()
    o_recv[xc] = o_send[xc]
    s_recv[xc] = s_send[xc]
    for d in range(1, XC):
        s_copy(d).wait_recv()
        o_copy(d).wait_recv()
    for h in range(4):
        lo, hi = HEAD_ROWS[h]
        tops = [s_recv[j, h : h + 1, :] for j in range(XC)]
        top = functools.reduce(jnp.maximum, tops)
        shares = [jnp.exp2(tops[j] - top) * s_recv[j, 4 + h : 5 + h, :] for j in range(XC)]
        whole = functools.reduce(jnp.add, shares)
        mixed = functools.reduce(
            jnp.add, [o_recv[j, lo:hi, :].astype(jnp.float32) * (shares[j] / whole) for j in range(XC)]
        )
        out_ref[lo:hi, :] = mixed.astype(jnp.bfloat16)

    q_sibling().wait_send()
    for d in range(1, 4):
        q_direct(d).wait_send()
        q_forward(d).wait_send()
    for s in range(1, 5):

        @pl.when(up_sends(s))
        def _(s=s):
            up_copy(s).wait_send()

    for s in range(1, 4):

        @pl.when(dn_sends(s))
        def _(s=s):
            dn_copy(s).wait_send()

    for d in range(1, XC):
        s_copy(d).wait_send()
        o_copy(d).wait_send()


def attention(query_wide, query_narrow, latent, rope_key, gain, wbk, wbv, wsk, wsv):
    position = lax.axis_index("sp") * BLOCK + jnp.arange(BLOCK, dtype=jnp.int32)
    angle = angles(position, ROPE)
    cos = jnp.tile(jnp.cos(angle), (1, 4))
    sin = jnp.sin(angle)
    sin = jnp.concatenate([-sin, sin, -sin, sin], axis=1)
    vmem = pl.BlockSpec(memory_space=pltpu.VMEM)
    bf16, f32, dma = jnp.bfloat16, jnp.float32, pltpu.SemaphoreType.DMA
    return pl.pallas_call(
        attention_kernel,
        out_shape=jax.ShapeDtypeStruct((384, BLOCK), bf16),
        in_specs=[vmem] * 11,
        out_specs=vmem,
        scratch_shapes=[
            pltpu.VMEM((XC, BLOCK, 640), bf16),
            pltpu.VMEM((Z, BLOCK, 640), bf16),
            pltpu.VMEM((BLOCK, 768), bf16),
            pltpu.VMEM((384, BLOCK), bf16),
            pltpu.VMEM((4, 384, 256), f32),
            pltpu.VMEM((4, 8, 256), f32),
            pltpu.VMEM((4, 8, 256), f32),
            pltpu.VMEM((XC, 384, BLOCK), bf16),
            pltpu.VMEM((XC, 384, BLOCK), bf16),
            pltpu.VMEM((XC, 8, BLOCK), f32),
            pltpu.VMEM((XC, 8, BLOCK), f32),
            dma((7,)), dma((7,)), dma((6,)), dma((6,)), dma((6,)), dma((6,)),
            dma((8,)), dma((8,)), dma((8,)), dma((8,)),
        ],
        compiler_params=pltpu.CompilerParams(collective_id=0, has_side_effects=True),
        name="attention",
    )(
        query_wide, query_narrow, latent, jnp.concatenate([rope_key, rope_key], axis=1), gain[None, :],
        wbk, wbv, wsk, wsv, cos, sin,
    )


def body(
    query_wide,
    query_narrow,
    latent,
    rope_key,
    latent_norm_weight,
    broad_key_lift,
    broad_value_lift,
    slim_key_lift,
    slim_value_lift,
    out_wide,
    out_narrow,
    resid,
    ffn_gain,
    group_route,
    expert_pair,
    group_prob,
    expert_prob,
    gate_weight,
    up_weight,
    down_weight,
):
    local_tokens = latent.shape[0]
    att = attention(
        query_wide, query_narrow, latent, rope_key, latent_norm_weight,
        broad_key_lift, broad_value_lift, slim_key_lift, slim_value_lift,
    )
    partial_value = lax.dot_general(
        att, jnp.concatenate([out_wide, out_narrow], axis=0), (((0,), (0,)), ((), ())),
        preferred_element_type=jnp.float32,
    )
    model_width = resid.shape[1]
    tp_size = lax.axis_size("tp")
    quarter = model_width // tp_size
    col_start = lax.axis_index("tp") * quarter
    share = sum_at_owner(partial_value.astype(jnp.bfloat16), "tp", 1)
    resid_cols = lax.dynamic_slice_in_dim(resid, col_start, quarter, 1)
    stream_cols = (resid_cols.astype(jnp.float32) + share).astype(jnp.bfloat16)
    widened = stream_cols.astype(jnp.float32)
    square_total = of_everyone(jnp.sum(widened * widened, axis=1), "tp")
    gain_cols = lax.dynamic_slice_in_dim(ffn_gain, col_start, quarter, 0)
    normed_cols = (
        widened * lax.rsqrt(square_total[:, None] / model_width + EPSILON) * gain_cols[None, :]
    ).astype(jnp.bfloat16)
    groups = lax.axis_size("sp")
    capacity = 2 * local_tokens // groups
    share_of = group_prob[:, None] * expert_prob / jnp.sum(expert_prob, axis=1, keepdims=True)
    chosen = (expert_pair[:, :, None] == jnp.arange(EPG, dtype=jnp.int32)[None, None, :]).astype(
        jnp.float32
    )
    combine = jnp.sum(share_of[:, :, None] * chosen, axis=1).astype(jnp.bfloat16)
    member = (group_route[:, None] == jnp.arange(groups, dtype=jnp.int32)[None, :]).astype(
        jnp.int32
    )
    group_rank = jnp.sum(jnp.cumsum(member, axis=0) * member, axis=1) - 1
    slot_index = group_route * capacity + group_rank
    routed_weights = jnp.zeros((groups * capacity, EPG), jnp.bfloat16).at[slot_index].set(combine)
    routed_weights = routed_weights.reshape(groups, capacity, EPG)
    placed = (
        jnp.zeros((groups * capacity, normed_cols.shape[1]), jnp.bfloat16)
        .at[slot_index]
        .set(normed_cols)
    )
    joined = gathered_copies(
        lax.all_to_all(
            placed.reshape(groups, capacity, normed_cols.shape[1]),
            "sp",
            split_axis=0,
            concat_axis=0,
            tiled=True,
        ),
        "tp",
        2,
    )
    slot_count = joined.shape[0] * joined.shape[1]
    flat_rows = joined.reshape(slot_count, joined.shape[2])
    gate_act = jnp.einsum(
        "rd,edf->ref", flat_rows, gate_weight[0], preferred_element_type=jnp.float32
    )
    up_act = jnp.einsum("rd,edf->ref", flat_rows, up_weight[0], preferred_element_type=jnp.float32)
    scaled = (
        lax.all_to_all(routed_weights, "sp", split_axis=0, concat_axis=0, tiled=True)
        .reshape(slot_count, EPG)
        .astype(jnp.float32)[:, :, None]
    )
    hidden = (jax.nn.silu(gate_act) * up_act * scaled).astype(jnp.bfloat16)
    partials = jnp.einsum("ref,efd->rd", hidden, down_weight[0], preferred_element_type=jnp.float32)
    partials = partials.reshape(joined.shape)
    summed_rows = sum_at_owner(partials.astype(jnp.bfloat16), "tp", 2).astype(jnp.bfloat16)
    returned_rows = lax.all_to_all(summed_rows, "sp", split_axis=0, concat_axis=0, tiled=True)
    moe_rows = returned_rows.reshape(groups * capacity, quarter)[slot_index]
    return (stream_cols.astype(jnp.float32) + moe_rows.astype(jnp.float32)).astype(jnp.bfloat16)


def solution(mesh):
    placed = (
        P("sp", "tp"),
        P("sp", "tp"),
        P("sp", None),
        P("sp", None),
        P(),
        P(None, "tp"),
        P(None, "tp"),
        P(None, "tp"),
        P(None, "tp"),
        P("tp", None),
        P("tp", None),
        P("sp", None),
        P(),
        P("sp"),
        P("sp", None),
        P("sp"),
        P("sp", None),
        P("sp", None, None, "tp"),
        P("sp", None, None, "tp"),
        P("sp", None, "tp", None),
    )
    return jax.shard_map(body, mesh=mesh, in_specs=placed, out_specs=P("sp", "tp"), check_vma=False)
```

```python
import functools

import jax
import jax.numpy as jnp
from jax import lax
from jax.experimental import pallas as pl
from jax.experimental.pallas import tpu as pltpu
from jax.sharding import PartitionSpec as P

PLAIN_WIDTH_WIDE = 128
PLAIN_WIDTH_SLIM = 64
ROPE = 64
VALUE_WIDTH_WIDE = 128
VALUE_WIDTH_SLIM = 64
EPG = 4


ROPE_BASE = 10000.0
EPSILON = 1e-06
MASKED = -1e30


def angles(positions, width):
    frequency = 1.0 / ROPE_BASE ** (jnp.arange(0, width, 2).astype(jnp.float32) / width)
    return positions.astype(jnp.float32)[:, None] * frequency[None, :]


MESH = pl.DeviceIdType.MESH
LOG2E = 1.4426950408889634
Z = 8
XC = 8
BLOCK = 128
HEAD_ROWS = ((0, 128), (128, 256), (256, 320), (320, 384))
HEAD_QUERY = ((0, 256), (128, 384), (384, 512), (512, 640))
HEAD_KEY = ((0, 256), (256, 512), (512, 640), (640, 768))
HEAD_SCALE = (192**-0.5 * LOG2E, 192**-0.5 * LOG2E, 128**-0.5 * LOG2E, 128**-0.5 * LOG2E)


def nt(a, b):
    return lax.dot_general(a, b, (((1,), (1,)), ((), ())), preferred_element_type=jnp.float32)


def nn(a, b):
    return lax.dot_general(a, b, (((1,), (0,)), ((), ())), preferred_element_type=jnp.float32)


def remote(src, dst, send_sem, recv_sem, sp):
    return pltpu.make_async_remote_copy(
        src_ref=src,
        dst_ref=dst,
        send_sem=send_sem,
        recv_sem=recv_sem,
        device_id={"sp": sp},
        device_id_type=MESH,
    )


def attention_kernel(
    qw_ref, qn_ref, latent_ref, rope_ref, gain_ref, wbk_ref, wbv_ref, wsk_ref, wsv_ref, cos_ref, sin_ref,
    out_ref,
    q_all, lat_all, keys, values, acc, peak, total, o_send, o_recv, s_send, s_recv,
    q_ssem, q_rsem, up_ssem, up_rsem, dn_ssem, dn_rsem, o_ssem, o_rsem, t_ssem, t_rsem,
):
    sp = lax.axis_index("sp")
    z = sp // XC
    xc = lax.rem(sp, XC)
    core = lax.rem(xc, 2)
    base = z * XC
    sibling = base + xc + 1 - 2 * core
    above = lax.rem(sp + XC, Z * XC)
    below = lax.rem(sp + (Z - 1) * XC, Z * XC)

    barrier = pltpu.get_barrier_semaphore()
    for d in range(1, XC):
        pl.semaphore_signal(barrier, inc=1, device_id={"sp": base + lax.rem(xc + d, XC)}, device_id_type=MESH)
    for peer in (above, below):
        pl.semaphore_signal(barrier, inc=1, device_id={"sp": peer}, device_id_type=MESH)

    lane = lax.broadcasted_iota(jnp.int32, (BLOCK, 128), 1)
    low = lane < 64
    first = lax.rem(lane, 64) < 32
    cos = cos_ref[...]
    sin = sin_ref[...]

    def turned(x):
        swapped = jnp.where(first, pltpu.roll(x, 96, 1), pltpu.roll(x, 32, 1))
        return x * cos + swapped * sin

    q_all[xc, :, 0:128] = qw_ref[:, 0:128]
    middle = qw_ref[:, 128:256].astype(jnp.float32)
    last = qw_ref[:, 256:384].astype(jnp.float32)
    q_all[xc, :, 128:256] = turned(jnp.where(low, middle, last)).astype(jnp.bfloat16)
    q_all[xc, :, 256:384] = pltpu.roll(jnp.where(low, last, middle), 64, 1).astype(jnp.bfloat16)
    for k in range(2):
        x = qn_ref[:, k * 128 : (k + 1) * 128].astype(jnp.float32)
        q_all[xc, :, 384 + k * 128 : 512 + k * 128] = jnp.where(low, x, turned(x)).astype(jnp.bfloat16)
    x = latent_ref[...].astype(jnp.float32)
    x = x * lax.rsqrt(jnp.mean(x * x, axis=1, keepdims=True) + EPSILON) * gain_ref[...]
    lat_all[z, :, 0:512] = x.astype(jnp.bfloat16)
    lat_all[z, :, 512:640] = turned(rope_ref[...].astype(jnp.float32)).astype(jnp.bfloat16)

    pl.semaphore_wait(barrier, XC + 1)

    def q_direct(d):
        return remote(
            q_all.at[xc], q_all.at[xc], q_ssem.at[d], q_rsem.at[d], base + lax.rem(xc + 2 * d, XC)
        )

    def q_sibling():
        return remote(q_all.at[xc], q_all.at[xc], q_ssem.at[0], q_rsem.at[0], sibling)

    def q_forward(d):
        slot = lax.rem(xc + 2 * (4 - d), XC)
        return remote(q_all.at[slot], q_all.at[slot], q_ssem.at[3 + d], q_rsem.at[3 + d], sibling)

    def up_copy(s):
        slot = lax.rem(z - s + 1 + Z, Z)
        return remote(lat_all.at[slot], lat_all.at[slot], up_ssem.at[s], up_rsem.at[s], above)

    def dn_copy(s):
        slot = lax.rem(z + s - 1, Z)
        return remote(lat_all.at[slot], lat_all.at[slot], dn_ssem.at[s], dn_rsem.at[s], below)

    def up_sends(s):
        return (s <= 4) & (z - s + 1 >= 0) & (z < Z - 1)

    def up_comes(s):
        return z - s >= 0

    def dn_sends(s):
        return (s <= 3) & (lax.rem(z + s - 1, Z) <= 2)

    def dn_comes(s):
        return (s <= 3) & (lax.rem(z + s, Z) <= 2)

    def start_step(s):
        @pl.when(up_sends(s))
        def _():
            up_copy(s).start()

        @pl.when(dn_sends(s))
        def _():
            dn_copy(s).start()

    def arrive_step(s):
        @pl.when(up_comes(s))
        def _():
            up_copy(s).wait_recv()

        @pl.when(dn_comes(s))
        def _():
            dn_copy(s).wait_recv()

    start_step(1)
    q_sibling().start()
    for d in range(1, 4):
        q_direct(d).start()

    peak[...] = jnp.full(peak.shape, MASKED, jnp.float32)
    total[...] = jnp.zeros(total.shape, jnp.float32)
    acc[...] = jnp.zeros(acc.shape, jnp.float32)

    def project(slot):
        rows = lat_all[slot, :, 0:512]
        rot = lat_all[slot, :, 512:640]
        wide = nn(rows, wbk_ref[...]).astype(jnp.bfloat16)
        zero = jnp.zeros_like(rot)
        keys[:, 0:128] = wide[:, 0:128]
        keys[:, 128:256] = jnp.where(low, rot, zero)
        keys[:, 256:384] = jnp.where(low, zero, rot)
        keys[:, 384:512] = wide[:, 128:256]
        slim = nn(rows, wsk_ref[...])
        keys[:, 512:640] = jnp.where(low, slim.astype(jnp.bfloat16), rot)
        keys[:, 640:768] = jnp.where(low, pltpu.roll(slim, 64, 1).astype(jnp.bfloat16), rot)
        values[0:256, :] = jnp.transpose(nn(rows, wbv_ref[...])).astype(jnp.bfloat16)
        values[256:384, :] = jnp.transpose(nn(rows, wsv_ref[...])).astype(jnp.bfloat16)

    def attend(slot, own):
        project(slot)

        def chunk(c, carry):
            if own:
                key_pos = xc * BLOCK + lax.broadcasted_iota(jnp.int32, (BLOCK, 256), 0)
                query_pos = c * 256 + lax.broadcasted_iota(jnp.int32, (BLOCK, 256), 1)
                seen = key_pos <= query_pos
            for h in range(4):
                ql, qh = HEAD_QUERY[h]
                kl, kh = HEAD_KEY[h]
                lo, hi = HEAD_ROWS[h]
                q = q_all[pl.ds(2 * c, 2), :, ql:qh].reshape(256, qh - ql)
                scores = nt(keys[:, kl:kh], q) * HEAD_SCALE[h]
                if own:
                    scores = jnp.where(seen, scores, MASKED)
                before = peak[c, h : h + 1, :]
                top = jnp.maximum(before, jnp.max(scores, axis=0, keepdims=True))
                keep = jnp.exp2(before - top)
                weights = jnp.exp2(scores - top)
                peak[c, h : h + 1, :] = top
                total[c, h : h + 1, :] = total[c, h : h + 1, :] * keep + jnp.sum(weights, axis=0, keepdims=True)
                acc[c, lo:hi, :] = acc[c, lo:hi, :] * keep + nn(values[lo:hi, :], weights.astype(jnp.bfloat16))
            return carry

        lax.fori_loop(0, 4, chunk, 0)

    arrive_step(1)
    start_step(2)
    for d in range(1, 4):
        q_direct(d).wait_recv()
        q_forward(d).start()
    q_sibling().wait_recv()
    for d in range(1, 4):
        q_forward(d).wait_recv()
    attend(z, True)

    def step(s, carry):
        @pl.when(s > 1)
        def _():
            arrive_step(s)
            start_step(s + 1)

        @pl.when(z - s >= 0)
        def _():
            attend(z - s, False)

        @pl.when((s <= 3) & (z + s >= Z))
        def _():
            attend(z + s - Z, False)

        return carry

    lax.fori_loop(1, 5, step, 0)

    for j in range(XC):
        c, lanes = j // 2, slice((j % 2) * 128, (j % 2) * 128 + 128)
        for h in range(4):
            lo, hi = HEAD_ROWS[h]
            o_send[j, lo:hi, :] = (acc[c, lo:hi, lanes] / total[c, h : h + 1, lanes]).astype(jnp.bfloat16)
            s_send[j, h : h + 1, :] = peak[c, h : h + 1, lanes]
            s_send[j, 4 + h : 5 + h, :] = total[c, h : h + 1, lanes]

    def o_copy(d):
        j = lax.rem(xc + d, XC)
        return remote(o_send.at[j], o_recv.at[xc], o_ssem.at[d], o_rsem.at[d], base + j)

    def s_copy(d):
        j = lax.rem(xc + d, XC)
        return remote(s_send.at[j], s_recv.at[xc], t_ssem.at[d], t_rsem.at[d], base + j)

    for d in range(1, XC):
        s_copy(d).start()
        o_copy(d).start()
    o_recv[xc] = o_send[xc]
    s_recv[xc] = s_send[xc]
    for d in range(1, XC):
        s_copy(d).wait_recv()
        o_copy(d).wait_recv()
    for h in range(4):
        lo, hi = HEAD_ROWS[h]
        tops = [s_recv[j, h : h + 1, :] for j in range(XC)]
        top = functools.reduce(jnp.maximum, tops)
        shares = [jnp.exp2(tops[j] - top) * s_recv[j, 4 + h : 5 + h, :] for j in range(XC)]
        whole = functools.reduce(jnp.add, shares)
        mixed = functools.reduce(
            jnp.add, [o_recv[j, lo:hi, :].astype(jnp.float32) * (shares[j] / whole) for j in range(XC)]
        )
        acc[0, lo:hi, 0:128] = mixed
    for k in range(3):
        out_ref[:, k * 128 : (k + 1) * 128] = jnp.transpose(acc[0, k * 128 : (k + 1) * 128, 0:128]).astype(jnp.bfloat16)

    q_sibling().wait_send()
    for d in range(1, 4):
        q_direct(d).wait_send()
        q_forward(d).wait_send()
    for s in range(1, 5):

        @pl.when(up_sends(s))
        def _(s=s):
            up_copy(s).wait_send()

    for s in range(1, 4):

        @pl.when(dn_sends(s))
        def _(s=s):
            dn_copy(s).wait_send()

    for d in range(1, XC):
        s_copy(d).wait_send()
        o_copy(d).wait_send()


def attention(query_wide, query_narrow, latent, rope_key, gain, wbk, wbv, wsk, wsv):
    position = lax.axis_index("sp") * BLOCK + jnp.arange(BLOCK, dtype=jnp.int32)
    angle = angles(position, ROPE)
    cos = jnp.tile(jnp.cos(angle), (1, 4))
    sin = jnp.sin(angle)
    sin = jnp.concatenate([-sin, sin, -sin, sin], axis=1)
    vmem = pl.BlockSpec(memory_space=pltpu.VMEM)
    bf16, f32, dma = jnp.bfloat16, jnp.float32, pltpu.SemaphoreType.DMA
    return pl.pallas_call(
        attention_kernel,
        out_shape=jax.ShapeDtypeStruct((BLOCK, 384), bf16),
        in_specs=[vmem] * 11,
        out_specs=vmem,
        scratch_shapes=[
            pltpu.VMEM((XC, BLOCK, 640), bf16),
            pltpu.VMEM((Z, BLOCK, 640), bf16),
            pltpu.VMEM((BLOCK, 768), bf16),
            pltpu.VMEM((384, BLOCK), bf16),
            pltpu.VMEM((4, 384, 256), f32),
            pltpu.VMEM((4, 8, 256), f32),
            pltpu.VMEM((4, 8, 256), f32),
            pltpu.VMEM((XC, 384, BLOCK), bf16),
            pltpu.VMEM((XC, 384, BLOCK), bf16),
            pltpu.VMEM((XC, 8, BLOCK), f32),
            pltpu.VMEM((XC, 8, BLOCK), f32),
            dma((7,)), dma((7,)), dma((6,)), dma((6,)), dma((6,)), dma((6,)),
            dma((8,)), dma((8,)), dma((8,)), dma((8,)),
        ],
        compiler_params=pltpu.CompilerParams(collective_id=0, has_side_effects=True),
        name="attention",
    )(
        query_wide, query_narrow, latent, jnp.concatenate([rope_key, rope_key], axis=1), gain[None, :],
        wbk, wbv, wsk, wsv, cos, sin,
    )


def tail_kernel(
    att_ref, ow_ref, on_ref, resid_ref, gain_ref, place_ref, cw_ref, gate_hbm, up_hbm, down_hbm,
    out_ref,
    gate, up, down, own, stream, far_s, far_r, near_s, comb_s, lb, rb, ss_s, ss_r,
    cx_s, cx_r, cz_s, cz_r, x_s, x_r, z_s, xg, hidden, part, mfar, mcomb, ml, mr, rz_s, rz_r, rx_s, rx_r,
    w_sem, p_ss, p_rs, q_ss, q_rs, cx_ss, cx_rs, cz_ss, cz_rs, x_ss, x_rs, z_ss, z_rs,
    gr_ss, gr_rs, gl_ss, gl_rs, gf_ss, gf_rs, mf_ss, mf_rs, mp_ss, mp_rs, mc_ss, mc_rs,
    rz_ss, rz_rs, rx_ss, rx_rs,
):
    sp = lax.axis_index("sp")
    tp = lax.axis_index("tp")
    z = sp // XC
    xc = lax.rem(sp, XC)
    right, left, far = lax.rem(tp + 1, 4), lax.rem(tp + 3, 4), lax.rem(tp + 2, 4)

    def x_peer(d):
        return {"sp": z * XC + lax.rem(xc + d, XC)}

    def z_peer(d):
        return {"sp": lax.rem(z + d, Z) * XC + xc}

    def send(src, dst, ssem, rsem, to):
        return pltpu.make_async_remote_copy(
            src_ref=src, dst_ref=dst, send_sem=ssem, recv_sem=rsem, device_id=to, device_id_type=MESH
        )

    weights = [
        pltpu.make_async_copy(gate_hbm, gate, w_sem.at[0]),
        pltpu.make_async_copy(up_hbm, up, w_sem.at[1]),
        pltpu.make_async_copy(down_hbm, down, w_sem.at[2]),
    ]
    barrier = pltpu.get_barrier_semaphore()
    for to in (right, left, far):
        pl.semaphore_signal(barrier, inc=1, device_id={"tp": to}, device_id_type=MESH)
    for d in range(1, XC):
        pl.semaphore_signal(barrier, inc=1, device_id=x_peer(d), device_id_type=MESH)
        pl.semaphore_signal(barrier, inc=1, device_id=z_peer(d), device_id_type=MESH)
    for copy in weights:
        copy.start()

    bf16, f32 = jnp.bfloat16, jnp.float32
    sent = []

    def go(copy):
        copy.start()
        sent.append(copy)

    def columns(q):
        return pl.ds(pl.multiple_of(q * 512, 512), 512)

    def quarter(q):
        return nn(att_ref[:, 0:256], ow_ref[:, columns(q)]) + nn(att_ref[:, 256:384], on_ref[:, columns(q)])

    far_s[...] = quarter(far).astype(bf16).reshape(far_s.shape)
    pl.semaphore_wait(barrier, 3 + 2 * (XC - 1))

    go(send(far_s.at[0], far_r.at[0], p_ss.at[0], p_rs.at[0], {"tp": right}))
    go(send(far_s.at[1], far_r.at[1], p_ss.at[1], p_rs.at[1], {"tp": left}))
    near_s[0] = quarter(right).astype(bf16).reshape(2, 64, 512)
    to_right = send(near_s.at[0, 1], lb.at[1], p_ss.at[2], p_rs.at[2], {"tp": right})
    go(to_right)
    near_s[1] = quarter(left).astype(bf16).reshape(2, 64, 512)
    to_left = send(near_s.at[1, 0], rb.at[0], p_ss.at[3], p_rs.at[3], {"tp": left})
    go(to_left)

    row = lax.broadcasted_iota(jnp.int32, (256, 256), 0)
    col = lax.broadcasted_iota(jnp.int32, (256, 256), 1)
    swap = (col == lax.rem(row // 4, 8) * 32 + (row // 32) * 4 + lax.rem(row, 4)).astype(f32).astype(bf16)

    def swapped(block):
        return nn(swap, block.reshape(256, block.shape[-1])).astype(bf16).reshape(block.shape)

    cx_s[...] = nn(place_ref[...], cw_ref[...]).astype(bf16).reshape(cx_s.shape)
    for d in range(1, XC):
        go(send(cx_s.at[d], cx_r.at[d], cx_ss.at[d], cx_rs.at[d], x_peer(d)))
    cx_r[0] = cx_s[0]

    own[...] = quarter(tp)
    far_right = send(far_s.at[0], far_r.at[0], p_ss.at[0], p_rs.at[0], {"tp": right})
    far_right.wait_recv()
    comb_s[0] = (far_r[0].astype(f32) + near_s[0, 0].astype(f32)).astype(bf16)
    comb_right = send(comb_s.at[0], lb.at[0], p_ss.at[4], p_rs.at[4], {"tp": right})
    go(comb_right)
    far_left = send(far_s.at[1], far_r.at[1], p_ss.at[1], p_rs.at[1], {"tp": left})
    far_left.wait_recv()
    comb_s[1] = (far_r[1].astype(f32) + near_s[1, 1].astype(f32)).astype(bf16)
    comb_left = send(comb_s.at[1], rb.at[1], p_ss.at[5], p_rs.at[5], {"tp": left})
    go(comb_left)

    for d in range(1, XC):
        send(cx_s.at[d], cx_r.at[d], cx_ss.at[d], cx_rs.at[d], x_peer(d)).wait_recv()
    cz_s[...] = swapped(cx_r[...])
    for d in range(1, Z):
        go(send(cz_s.at[d], cz_r.at[d], cz_ss.at[d], cz_rs.at[d], z_peer(d)))
    cz_r[0] = cz_s[0]

    for copy in (to_right, to_left, comb_right, comb_left):
        copy.wait_recv()
    share = lb[...].astype(f32).reshape(128, 512) + rb[...].astype(f32).reshape(128, 512) + own[...]
    rounded = (resid_ref[:, columns(tp)].astype(f32) + share).astype(bf16)
    stream[...] = rounded.astype(f32)
    widened = stream[...]
    squares = jnp.sum(widened * widened, axis=1, keepdims=True)
    ss_s[...] = jnp.transpose(jnp.broadcast_to(squares, (128, 128)))[0:8, :]
    squared = [
        send(ss_s, ss_r.at[k], q_ss.at[k], q_rs.at[k], {"tp": to}) for k, to in enumerate((right, left, far))
    ]
    for copy in squared:
        go(copy)
    for copy in squared:
        copy.wait_recv()
    squares = ss_s[0:1, :] + ss_r[0, 0:1, :] + ss_r[1, 0:1, :] + ss_r[2, 0:1, :]
    squares = jnp.transpose(jnp.broadcast_to(squares, (128, 128)))[:, 0:1]
    normed = stream[...] * lax.rsqrt(squares / 2048.0 + EPSILON) * gain_ref[:, columns(tp)]
    x_s[...] = nn(place_ref[...], normed.astype(bf16)).astype(bf16).reshape(x_s.shape)

    for d in (4, 3, 5, 2, 6, 7, 1):
        go(send(x_s.at[d], x_r.at[d], x_ss.at[d], x_rs.at[d], x_peer(d)))
    x_r[0] = x_s[0]
    for d in range(1, XC):
        send(x_s.at[d], x_r.at[d], x_ss.at[d], x_rs.at[d], x_peer(d)).wait_recv()
    z_s[...] = swapped(x_r[...])
    for d in (1, 7, 2, 6, 3, 5, 4):
        go(send(z_s.at[d], xg.at[0, d], z_ss.at[d], z_rs.at[d], z_peer(d)))
    xg[0, 0] = z_s[0]

    order = (0, 1, 7, 2, 6, 3, 5, 4)

    def gather_right(d):
        return send(xg.at[0, d], xg.at[1, d], gr_ss.at[d], gr_rs.at[d], {"tp": right})

    def gather_left(d):
        return send(xg.at[0, d], xg.at[3, d], gl_ss.at[d], gl_rs.at[d], {"tp": left})

    def gather_far(n):
        d = order[n]
        if n % 2 == 0:
            return send(xg.at[1, d], xg.at[2, d], gf_ss.at[d], gf_rs.at[d], {"tp": right})
        return send(xg.at[3, d], xg.at[2, d], gf_ss.at[d], gf_rs.at[d], {"tp": left})

    def pass_on(n):
        if n % 2 == 0:
            gather_right(order[n]).wait_recv()
        else:
            gather_left(order[n]).wait_recv()
        go(gather_far(n))

    for n, d in enumerate(order):
        if d:
            send(z_s.at[d], xg.at[0, d], z_ss.at[d], z_rs.at[d], z_peer(d)).wait_recv()
        go(gather_right(d))
        go(gather_left(d))
        if n >= 1:
            pass_on(n - 1)
    pass_on(7)
    for d in range(1, Z):
        send(cz_s.at[d], cz_r.at[d], cz_ss.at[d], cz_rs.at[d], z_peer(d)).wait_recv()
    for copy in weights:
        copy.wait()
    for n, d in enumerate(order):
        if n % 2 == 0:
            gather_left(d).wait_recv()
        else:
            gather_right(d).wait_recv()
        gather_far(n).wait_recv()

    rows_of = (tp, left, far, right)
    scale = cz_r[...].reshape(256, 128).astype(f32)
    for e in range(EPG):
        both = jnp.zeros((256, 256), f32)
        for k in range(4):
            rows = pl.ds(pl.multiple_of(rows_of[k] * 512, 512), 512)
            both = both + nn(
                xg[k].reshape(256, 512), jnp.concatenate([gate[e, rows, :], up[e, rows, :]], axis=1)
            )
        g = both[:, 0:128]
        active = g / (1.0 + jnp.exp(-g)) * both[:, 128:256] * scale[:, e : e + 1]
        hidden[:, e * 128 : (e + 1) * 128] = active.astype(bf16)

    def expert_out(q):
        return nn(hidden[...], down[:, :, columns(q)].reshape(512, 512)).astype(bf16).reshape(8, 32, 512)

    back = (4, 3, 5, 2, 6, 1, 7, 0)

    def m_far(n):
        to = right if n % 2 == 0 else left
        d = back[n]
        return send(part.at[2, d], mfar.at[d], mf_ss.at[d], mf_rs.at[d], {"tp": to})

    def m_plain(n):
        d = back[n]
        if n % 2 == 0:
            return send(part.at[3, d], mr.at[d], mp_ss.at[d], mp_rs.at[d], {"tp": left})
        return send(part.at[1, d], ml.at[d], mp_ss.at[d], mp_rs.at[d], {"tp": right})

    def m_comb(n):
        d = back[n]
        if n % 2 == 0:
            return send(mcomb.at[d], ml.at[d], mc_ss.at[d], mc_rs.at[d], {"tp": right})
        return send(mcomb.at[d], mr.at[d], mc_ss.at[d], mc_rs.at[d], {"tp": left})

    def z_back(d):
        return send(rz_s.at[d], rz_r.at[d], rz_ss.at[d], rz_rs.at[d], z_peer(Z - d))

    def x_back(d):
        return send(rx_s.at[d], rx_r.at[d], rx_ss.at[d], rx_rs.at[d], x_peer(XC - d))

    part[2] = expert_out(far)
    for n in range(8):
        go(m_far(n))
    part[1] = expert_out(right)
    part[3] = expert_out(left)
    for n in range(8):
        go(m_plain(n))
    part[0] = expert_out(tp)

    def combine_on(n):
        d = back[n]
        m_far(n).wait_recv()
        mcomb[d] = (mfar[d].astype(f32) + part[1 if n % 2 == 0 else 3, d].astype(f32)).astype(bf16)
        go(m_comb(n))

    def finish_chunk(n):
        d = back[n]
        m_plain(n).wait_recv()
        m_comb(n).wait_recv()
        total = (part[0, d].astype(f32) + ml[d].astype(f32) + mr[d].astype(f32)).astype(bf16)
        if d:
            rz_s[d] = total
            go(z_back(d))
        else:
            rz_r[0] = total

    for n in range(8):
        combine_on(n)
        if n >= 2:
            finish_chunk(n - 2)
    finish_chunk(6)
    finish_chunk(7)
    for d in range(1, Z):
        z_back(d).wait_recv()
    rx_s[...] = swapped(rz_r[...])
    for d in (4, 3, 5, 2, 6, 7, 1):
        go(x_back(d))
    rx_r[0] = rx_s[0]
    for d in range(1, XC):
        x_back(d).wait_recv()
    moe = lax.dot_general(
        place_ref[...], rx_r[...].reshape(256, 512), (((0,), (0,)), ((), ())), preferred_element_type=f32
    )
    out_ref[...] = (stream[...] + moe.astype(bf16).astype(f32)).astype(bf16)
    for copy in sent:
        copy.wait_send()


def tail(att, out_wide, out_narrow, resid, gain, place, combine, gate, up, down):
    vmem = pl.BlockSpec(memory_space=pltpu.VMEM)
    hbm = pl.BlockSpec(memory_space=pl.ANY)
    bf16, f32, dma = jnp.bfloat16, jnp.float32, pltpu.SemaphoreType.DMA

    def chunks(width, *lead):
        return pltpu.VMEM((*lead, 8, 32, width), bf16)

    half = pltpu.VMEM((2, 64, 512), bf16)
    return pl.pallas_call(
        tail_kernel,
        out_shape=jax.ShapeDtypeStruct((BLOCK, 512), bf16),
        in_specs=[vmem] * 7 + [hbm] * 3,
        out_specs=vmem,
        scratch_shapes=[
            pltpu.VMEM((4, 2048, 128), bf16), pltpu.VMEM((4, 2048, 128), bf16), pltpu.VMEM((4, 128, 2048), bf16),
            pltpu.VMEM((128, 512), f32), pltpu.VMEM((128, 512), f32),
            half, half, pltpu.VMEM((2, 2, 64, 512), bf16), half, half, half,
            pltpu.VMEM((8, 128), f32), pltpu.VMEM((3, 8, 128), f32),
            chunks(128), chunks(128), chunks(128), chunks(128),
            chunks(512), chunks(512), chunks(512), chunks(512, 4), pltpu.VMEM((256, 512), bf16), chunks(512, 4),
            chunks(512), chunks(512), chunks(512), chunks(512), chunks(512), chunks(512), chunks(512), chunks(512),
            dma((3,)), dma((6,)), dma((6,)), dma((3,)), dma((3,)),
            *[dma((8,))] * 24,
        ],
        compiler_params=pltpu.CompilerParams(
            collective_id=1, has_side_effects=True, vmem_limit_bytes=60 * 1024 * 1024
        ),
        name="tail",
    )(att, out_wide, out_narrow, resid, gain[None, :], place, combine, gate, up, down)


def body(
    query_wide,
    query_narrow,
    latent,
    rope_key,
    latent_norm_weight,
    broad_key_lift,
    broad_value_lift,
    slim_key_lift,
    slim_value_lift,
    out_wide,
    out_narrow,
    resid,
    ffn_gain,
    group_route,
    expert_pair,
    group_prob,
    expert_prob,
    gate_weight,
    up_weight,
    down_weight,
):
    local_tokens = latent.shape[0]
    att = attention(
        query_wide, query_narrow, latent, rope_key, latent_norm_weight,
        broad_key_lift, broad_value_lift, slim_key_lift, slim_value_lift,
    )
    token = jnp.arange(local_tokens, dtype=jnp.int32)
    same = group_route[:, None] == group_route[None, :]
    rank = jnp.sum((same & (token[None, :] < token[:, None])).astype(jnp.int32), axis=1)
    own_index = lax.axis_index("sp")
    dz = (group_route // XC - own_index // XC) % Z
    dx = (group_route % XC - own_index % XC) % XC
    slot_index = dx * 32 + dz * 4 + rank
    place = (jnp.arange(256, dtype=jnp.int32)[:, None] == slot_index[None, :]).astype(jnp.bfloat16)
    share_of = group_prob[:, None] * expert_prob / jnp.sum(expert_prob, axis=1, keepdims=True)
    chosen = (expert_pair[:, :, None] == jnp.arange(128, dtype=jnp.int32)[None, None, :]).astype(jnp.float32)
    combine = jnp.sum(share_of[:, :, None] * chosen, axis=1).astype(jnp.bfloat16)
    return tail(
        att, out_wide, out_narrow, resid, ffn_gain, place, combine, gate_weight[0], up_weight[0], down_weight[0]
    )


def solution(mesh):
    placed = (
        P("sp", "tp"),
        P("sp", "tp"),
        P("sp", None),
        P("sp", None),
        P(),
        P(None, "tp"),
        P(None, "tp"),
        P(None, "tp"),
        P(None, "tp"),
        P("tp", None),
        P("tp", None),
        P("sp", None),
        P(),
        P("sp"),
        P("sp", None),
        P("sp"),
        P("sp", None),
        P("sp", None, None, "tp"),
        P("sp", None, None, "tp"),
        P("sp", None, "tp", None),
    )
    return jax.shard_map(body, mesh=mesh, in_specs=placed, out_specs=P("sp", "tp"), check_vma=False)
```

```python
import functools

import jax
import jax.numpy as jnp
from jax import lax
from jax.experimental import pallas as pl
from jax.experimental.pallas import tpu as pltpu
from jax.sharding import PartitionSpec as P

PLAIN_WIDTH_WIDE = 128
PLAIN_WIDTH_SLIM = 64
ROPE = 64
VALUE_WIDTH_WIDE = 128
VALUE_WIDTH_SLIM = 64
EPG = 4


ROPE_BASE = 10000.0
EPSILON = 1e-06
MASKED = -1e30


MESH = pl.DeviceIdType.MESH
LOG2E = 1.4426950408889634
Z = 8
XC = 8
BLOCK = 128
A_COUNT = 38
ROWS = ((0, 128), (128, 192), (192, 320), (320, 384))
QUERY = ((0, 256), (384, 512), (128, 384), (512, 640))
KEY = ((0, 256), (512, 640), (256, 512), (640, 768))
WIDE_SCALE = (PLAIN_WIDTH_WIDE + ROPE) ** -0.5 * LOG2E
SLIM_SCALE = (PLAIN_WIDTH_SLIM + ROPE) ** -0.5 * LOG2E


def nt(a, b):
    return lax.dot_general(a, b, (((1,), (1,)), ((), ())), preferred_element_type=jnp.float32)


def nn(a, b):
    return lax.dot_general(a, b, (((1,), (0,)), ((), ())), preferred_element_type=jnp.float32)


def remote(src, dst, send_sem, recv_sem, sp):
    return pltpu.make_async_remote_copy(
        src_ref=src,
        dst_ref=dst,
        send_sem=send_sem,
        recv_sem=recv_sem,
        device_id={"sp": sp},
        device_id_type=MESH,
    )


def attention_part(
    go, entered, lifts,
    qw_ref, qn_ref, latent_ref, rope_ref, gain_ref, wbk_ref, wbv_ref, wsk_ref, wsv_ref, cos_ref, sin_ref,
    att_ref,
    q_all, lat_all, keys, values, acc, peak, total,
    b_s, bs_s, b_r, bs_r, g, gs, far_r, fars_r, comb, combs, lb, lbs, rb, rbs, own,
    q_ss, q_rs, qs_ss, qs_rs, up_ss, up_rs, dn_ss, dn_rs, b_ss, b_rs, bt_ss, bt_rs, o_ss, o_rs, t_ss, t_rs,
):
    bf16, f32 = jnp.bfloat16, jnp.float32
    sp = lax.axis_index("sp")
    z = sp // XC
    xc = lax.rem(sp, XC)
    x = xc // 2
    core = lax.rem(xc, 2)
    base = z * XC
    sibling = base + xc + 1 - 2 * core
    above = lax.rem(sp + XC, Z * XC)
    below = lax.rem(sp + (Z - 1) * XC, Z * XC)
    right = base + lax.rem(x + 1, 4) * 2 + core
    left = base + lax.rem(x + 3, 4) * 2 + core

    lane = lax.broadcasted_iota(jnp.int32, (BLOCK, 128), 1)
    low = lane < 64
    first = lax.rem(lane, 64) < 32
    cos = cos_ref[...]
    sin = sin_ref[...]

    def turned(v):
        swapped = jnp.where(first, pltpu.roll(v, 96, 1), pltpu.roll(v, 32, 1))
        return v * cos + swapped * sin

    v = latent_ref[...].astype(f32)
    v = (v * lax.rsqrt(jnp.mean(v * v, axis=1, keepdims=True) + EPSILON) * gain_ref[...]).astype(bf16)
    lat_all[z, :, 0:512] = v[0:64]
    lat_all[z, :, 512:1024] = v[64:128]
    rope = rope_ref[...].astype(f32)
    rope = turned(jnp.transpose(jnp.concatenate([rope, rope], axis=0)))
    lat_all[z, :, 1024:1152] = jnp.where(low[0:64], rope[0:64], rope[64:128]).astype(bf16)
    q_all[xc, :, 0:128] = qw_ref[:, 0:128]
    middle = qw_ref[:, 128:256].astype(f32)
    last = qw_ref[:, 256:384].astype(f32)
    q_all[xc, :, 128:256] = (turned(jnp.where(low, middle, last)) * WIDE_SCALE).astype(bf16)
    q_all[xc, :, 256:384] = pltpu.roll(jnp.where(low, last, middle), 64, 1).astype(bf16)
    for k in range(2):
        v = qn_ref[:, k * 128 : (k + 1) * 128].astype(f32)
        q_all[xc, :, 384 + k * 128 : 512 + k * 128] = jnp.where(low, v, turned(v) * SLIM_SCALE).astype(bf16)

    entered()

    def ring(slot, h, ssem, rsem, to):
        part = lat_all.at[slot, pl.ds(h * 32, 32)]
        return remote(part, part, ssem, rsem, to)

    def up_copy(s, h):
        return ring(lax.rem(z - s + 1 + Z, Z), h, up_ss.at[s, h], up_rs.at[s, h], above)

    def dn_copy(s, h):
        return ring(lax.rem(z + s - 1, Z), h, dn_ss.at[s, h], dn_rs.at[s, h], below)

    def up_sends(s):
        return (z - s + 1 >= 0) & (z < Z - 1)

    def up_comes(s):
        return z - s >= 0

    def dn_sends(s):
        return lax.rem(z + s - 1, Z) <= 2

    def dn_comes(s):
        return lax.rem(z + s, Z) <= 2

    def start_part(s, h):
        if s <= 4:

            @pl.when(up_sends(s))
            def _():
                up_copy(s, h).start()

        if s <= 3:

            @pl.when(dn_sends(s))
            def _():
                dn_copy(s, h).start()

    def hand_on(s):
        for h in range(2):

            @pl.when(up_comes(s))
            def _(h=h):
                up_copy(s, h).wait_recv()

            if s <= 3:

                @pl.when(dn_comes(s))
                def _(h=h):
                    dn_copy(s, h).wait_recv()

            start_part(s + 1, h)

    start_part(1, 0)
    start_part(1, 1)

    def q_part(slot, h, ssem, rsem, to):
        part = q_all.at[slot, pl.ds(h * 64, 64)]
        return remote(part, part, ssem, rsem, to)

    def x_slot(d):
        return lax.rem(x + d, 4) * 2 + core

    def q_right(h):
        return q_part(xc, h, q_ss.at[h], q_rs.at[h], right)

    def q_left(h):
        return q_part(xc, h, q_ss.at[2 + h], q_rs.at[2 + h], left)

    def q_on(h):
        if h == 0:
            return q_part(x_slot(3), 0, q_ss.at[4], q_rs.at[4], right)
        return q_part(x_slot(1), 1, q_ss.at[5], q_rs.at[5], left)

    def q_sibling(d, h):
        return q_part(x_slot(d), h, qs_ss.at[d, h], qs_rs.at[d, h], sibling)

    go(q_right(0))
    go(q_left(1))
    go(q_right(1))
    go(q_left(0))
    go(q_sibling(0, 0))
    go(q_sibling(0, 1))

    peak[...] = jnp.full(peak.shape, MASKED, f32)
    total[...] = jnp.zeros(total.shape, f32)
    acc[...] = jnp.zeros(acc.shape, f32)

    def project(slot):
        rows = jnp.concatenate([lat_all[slot, :, 0:512], lat_all[slot, :, 512:1024]], axis=0)
        packed = lat_all[slot, :, 1024:1152].astype(f32)
        other = pltpu.roll(packed, 64, 1)
        top = low[0:64]
        rot = jnp.concatenate([jnp.where(top, packed, other), jnp.where(top, other, packed)], axis=0)
        wide = (nn(rows, wbk_ref[...]) * WIDE_SCALE).astype(bf16)
        keys[slot, :, 0:128] = wide[:, 0:128]
        keys[slot, :, 128:256] = jnp.where(low, rot, 0.0).astype(bf16)
        keys[slot, :, 256:384] = jnp.where(low, 0.0, rot).astype(bf16)
        keys[slot, :, 384:512] = wide[:, 128:256]
        slim = nn(rows, wsk_ref[...]) * SLIM_SCALE
        keys[slot, :, 512:640] = jnp.where(low, slim, rot).astype(bf16)
        keys[slot, :, 640:768] = jnp.where(low, pltpu.roll(slim, 64, 1), rot).astype(bf16)
        wide = jnp.transpose(nn(rows, wbv_ref[...])).astype(bf16)
        slim = jnp.transpose(nn(rows, wsv_ref[...])).astype(bf16)
        values[slot, 0:128] = wide[0:128]
        values[slot, 128:192] = slim[0:64]
        values[slot, 192:320] = wide[128:256]
        values[slot, 320:384] = slim[64:128]

    def attend(slot, own_block):
        units = [(c, h) for c in range(4) for h in range(4)]

        def score(unit):
            c, h = unit
            ql, qh = QUERY[h]
            kl, kh = KEY[h]
            s = nt(keys[slot, :, kl:kh], q_all[2 * c : 2 * c + 2, :, ql:qh].reshape(256, qh - ql))
            if own_block:
                key_pos = xc * BLOCK + lax.broadcasted_iota(jnp.int32, (BLOCK, 256), 0)
                query_pos = c * 256 + lax.broadcasted_iota(jnp.int32, (BLOCK, 256), 1)
                s = jnp.where(key_pos <= query_pos, s, MASKED)
            return s

        coming = score(units[0])
        for n, (c, h) in enumerate(units):
            s = coming
            if n + 1 < len(units):
                coming = score(units[n + 1])
            lo, hi = ROWS[h]
            before = peak[c, h : h + 1, :]
            top = jnp.maximum(before, jnp.max(s, axis=0, keepdims=True))
            keep = jnp.exp2(before - top)
            weights = jnp.exp2(s - top)
            peak[c, h : h + 1, :] = top
            total[c, h : h + 1, :] = total[c, h : h + 1, :] * keep + jnp.sum(weights, axis=0, keepdims=True)
            acc[c, lo:hi, :] = acc[c, lo:hi, :] * keep + nn(values[slot, lo:hi, :], weights.astype(bf16))

    for copy in lifts:
        copy.wait()
    project(z)
    hand_on(1)
    q_right(0).wait_recv()
    go(q_on(0))
    q_left(1).wait_recv()
    go(q_on(1))
    go(q_sibling(3, 0))
    go(q_sibling(1, 1))
    q_right(1).wait_recv()
    go(q_sibling(3, 1))
    q_left(0).wait_recv()
    go(q_sibling(1, 0))
    hand_on(2)
    for h in range(2):
        q_on(h).wait_recv()
        go(q_sibling(2, h))

    def needed(i):
        s, up = i // 2 + 1, lax.rem(i, 2) == 0
        slot = jnp.where(up, z - s, z + s - Z)
        return slot, (slot >= 0) & (up | (s <= 3))

    def project_some(lo, hi):
        def some(i, carry):
            slot, wanted = needed(i)

            @pl.when(wanted)
            def _():
                project(slot)

            return carry

        lax.fori_loop(lo, hi, some, 0)

    project_some(0, 4)
    for d in (0, 1, 3, 2):
        for h in range(2):
            q_sibling(d, h).wait_recv()
    attend(z, True)
    hand_on(3)

    def visit(i, carry):
        slot, wanted = needed(i)

        @pl.when(i == 2)
        def _():
            hand_on(4)
            project_some(4, 7)

        @pl.when(wanted)
        def _():
            attend(slot, False)

        return carry

    lax.fori_loop(0, 7, visit, 0)

    def block_of(d, which):
        lanes = pl.ds(pl.multiple_of(which * 128, 128), 128)
        chip = lax.rem(x + d, 4)
        stats = jnp.concatenate([peak[chip, 0:4, lanes], total[chip, 0:4, lanes]], axis=0)
        return [acc[chip, lo:hi, lanes] / stats[4 + h : 5 + h, :] for h, (lo, hi) in enumerate(ROWS)], stats

    def merge(parts, heads=(0, 1, 2, 3)):
        results, tops, wholes = [], [], []
        for h in heads:
            top = functools.reduce(jnp.maximum, [stats[h : h + 1, :] for _, stats in parts])
            shares = [jnp.exp2(stats[h : h + 1, :] - top) * stats[4 + h : 5 + h, :] for _, stats in parts]
            whole = functools.reduce(jnp.add, shares)
            results.append(
                functools.reduce(jnp.add, [rows[h] * (share / whole) for (rows, _), share in zip(parts, shares)])
            )
            tops.append(top)
            wholes.append(whole)
        return results, tops, wholes

    def rows_of(ref):
        return [ref[lo:hi, :].astype(f32) for lo, hi in ROWS]

    def half_rows(ref, h):
        mine = {2 * h: ref[0:128, :].astype(f32), 2 * h + 1: ref[128:192, :].astype(f32)}
        return [mine.get(k) for k in range(4)]

    def b_copy(d):
        return remote(b_s.at[d], b_r.at[lax.rem(d + 0, 4)], b_ss.at[d], b_rs.at[d], sibling)

    def bs_copy(d):
        return remote(bs_s.at[d], bs_r.at[d], bt_ss.at[d], bt_rs.at[d], sibling)

    for d in (2, 1, 3, 0):
        rows, stats = block_of(d, 1 - core)
        bs_s[d] = stats
        for h, (lo, hi) in enumerate(ROWS):
            b_s[d, lo:hi, :] = rows[h].astype(bf16)
        go(bs_copy(d))
        go(b_copy(d))

    def pair(src, ssrc, dst, sdst, k, to):
        return (
            remote(ssrc, sdst, t_ss.at[k], t_rs.at[k], to),
            remote(src, dst, o_ss.at[k], o_rs.at[k], to),
        )

    def half(ref, d, h):
        return ref.at[d, pl.ds(h * 192, 192)]

    hops = [
        pair(half(g, 2, 0), gs.at[2], far_r.at[0], fars_r.at[0], 0, right),
        pair(half(g, 2, 1), gs.at[2], far_r.at[1], fars_r.at[1], 1, left),
        pair(half(g, 1, 1), gs.at[1], lb.at[1], lbs.at[1], 2, right),
        pair(half(g, 3, 0), gs.at[3], rb.at[0], rbs.at[0], 3, left),
        pair(comb.at[0], combs.at[0], lb.at[0], lbs.at[0], 4, right),
        pair(comb.at[1], combs.at[1], rb.at[1], rbs.at[1], 5, left),
    ]

    def start_hop(k):
        for copy in hops[k]:
            go(copy)

    def await_hop(k):
        for copy in hops[k]:
            copy.wait_recv()

    for d in (2, 1, 3, 0):
        bs_copy(d).wait_recv()
        b_copy(d).wait_recv()
        results, tops, wholes = merge([block_of(d, core), (rows_of(b_r.at[d]), bs_r[d])])
        gs[d] = jnp.concatenate(tops + wholes, axis=0)
        for h, (lo, hi) in enumerate(ROWS):
            if d == 0:
                own[lo:hi, :] = results[h]
            else:
                g[d, lo:hi, :] = results[h].astype(bf16)
        if d == 2:
            start_hop(0)
            start_hop(1)
        elif d == 1:
            start_hop(2)
        elif d == 3:
            start_hop(3)
    for h, d in ((0, 1), (1, 3)):
        await_hop(h)
        heads = (2 * h, 2 * h + 1)
        mine = half_rows(g.at[d, pl.ds(h * 192, 192)], h)
        results, tops, wholes = merge([(half_rows(far_r.at[h], h), fars_r[h]), (mine, gs[d])], heads)
        comb[h, 0:128, :] = results[0].astype(bf16)
        comb[h, 128:192, :] = results[1].astype(bf16)
        idle = jnp.zeros((2, 128), f32)
        tops, wholes = jnp.concatenate(tops, axis=0), jnp.concatenate(wholes, axis=0)
        order = [tops, idle, wholes, idle] if h == 0 else [idle, tops, idle, wholes]
        combs[h] = jnp.concatenate(order, axis=0)
        start_hop(4 + h)
    for k in range(2, 6):
        await_hop(k)
    final = []
    for h in range(2):
        mine = [own[lo:hi, :] for lo, hi in ROWS]
        results, _, _ = merge(
            [(mine, gs[0]), (half_rows(lb.at[h], h), lbs[h]), (half_rows(rb.at[h], h), rbs[h])], (2 * h, 2 * h + 1)
        )
        final.append(results)
    att_ref[:, 0:128] = jnp.transpose(final[0][0]).astype(bf16)
    att_ref[:, 128:256] = jnp.transpose(final[1][0]).astype(bf16)
    att_ref[:, 256:384] = jnp.transpose(jnp.concatenate([final[0][1], final[1][1]], axis=0)).astype(bf16)

    for s in range(1, 5):
        for h in range(2):

            @pl.when(up_sends(s))
            def _(s=s, h=h):
                up_copy(s, h).wait_send()

            if s <= 3:

                @pl.when(dn_sends(s))
                def _(s=s, h=h):
                    dn_copy(s, h).wait_send()


def tail_part(
    go, projections, weights,
    att_ref, ow_ref, on_ref, resid, gain_ref, place, cw, gate, up, down, stream_ref, moe_ref,
    own, far_s, far_r, near_s, comb_s, lb, rb, ss_s, ss_r,
    cx_s, cx_r, cz_s, cz_r, x_s, x_r, z_s, xg, hidden, part, mfar, mcomb, ml, mr, rz_s, rz_r, rx_s, rx_r,
    p_ss, p_rs, q_ss, q_rs, cx_ss, cx_rs, cz_ss, cz_rs, x_ss, x_rs, z_ss, z_rs,
    gr_ss, gr_rs, gl_ss, gl_rs, gf_ss, gf_rs, mf_ss, mf_rs, mp_ss, mp_rs, mc_ss, mc_rs,
    rz_ss, rz_rs, rx_ss, rx_rs,
):
    sp = lax.axis_index("sp")
    tp = lax.axis_index("tp")
    z = sp // XC
    xc = lax.rem(sp, XC)
    right, left, far = lax.rem(tp + 1, 4), lax.rem(tp + 3, 4), lax.rem(tp + 2, 4)

    def x_peer(d):
        return {"sp": z * XC + lax.rem(xc + d, XC)}

    def z_peer(d):
        return {"sp": lax.rem(z + d, Z) * XC + xc}

    def send(src, dst, ssem, rsem, to):
        return pltpu.make_async_remote_copy(
            src_ref=src, dst_ref=dst, send_sem=ssem, recv_sem=rsem, device_id=to, device_id_type=MESH
        )

    bf16, f32 = jnp.bfloat16, jnp.float32
    def columns(q):
        return pl.ds(pl.multiple_of(q * 512, 512), 512)

    def quarter(q):
        return nn(att_ref[:, 0:256], ow_ref[:, columns(q)]) + nn(att_ref[:, 256:384], on_ref[:, columns(q)])

    for copy in projections:
        copy.wait()
    far_s[...] = quarter(far).astype(bf16).reshape(far_s.shape)

    go(send(far_s.at[0], far_r.at[0], p_ss.at[0], p_rs.at[0], {"tp": right}))
    go(send(far_s.at[1], far_r.at[1], p_ss.at[1], p_rs.at[1], {"tp": left}))
    near_s[0] = quarter(right).astype(bf16).reshape(2, 64, 512)
    to_right = send(near_s.at[0, 1], lb.at[1], p_ss.at[2], p_rs.at[2], {"tp": right})
    go(to_right)
    near_s[1] = quarter(left).astype(bf16).reshape(2, 64, 512)
    to_left = send(near_s.at[1, 0], rb.at[0], p_ss.at[3], p_rs.at[3], {"tp": left})
    go(to_left)

    row = lax.broadcasted_iota(jnp.int32, (256, 256), 0)
    col = lax.broadcasted_iota(jnp.int32, (256, 256), 1)
    swap = (col == lax.rem(row // 4, 8) * 32 + (row // 32) * 4 + lax.rem(row, 4)).astype(f32).astype(bf16)

    def swapped(block):
        return nn(swap, block.reshape(256, block.shape[-1])).astype(bf16).reshape(block.shape)

    own[...] = quarter(tp)
    far_right = send(far_s.at[0], far_r.at[0], p_ss.at[0], p_rs.at[0], {"tp": right})
    far_right.wait_recv()
    comb_s[0] = (far_r[0].astype(f32) + near_s[0, 0].astype(f32)).astype(bf16)
    comb_right = send(comb_s.at[0], lb.at[0], p_ss.at[4], p_rs.at[4], {"tp": right})
    go(comb_right)
    far_left = send(far_s.at[1], far_r.at[1], p_ss.at[1], p_rs.at[1], {"tp": left})
    far_left.wait_recv()
    comb_s[1] = (far_r[1].astype(f32) + near_s[1, 1].astype(f32)).astype(bf16)
    comb_left = send(comb_s.at[1], rb.at[1], p_ss.at[5], p_rs.at[5], {"tp": left})
    go(comb_left)

    for copy in (to_right, to_left, comb_right, comb_left):
        copy.wait_recv()
    share = lb[...].astype(f32).reshape(128, 512) + rb[...].astype(f32).reshape(128, 512) + own[...]
    rounded = (resid[...].astype(f32) + share).astype(bf16)
    stream_ref[...] = rounded
    widened = rounded.astype(f32)
    scaled = (widened * gain_ref[:, columns(tp)]).astype(bf16)
    x_s[...] = nn(place[...], scaled).astype(bf16).reshape(x_s.shape)
    for d in (4, 3, 5, 2, 6, 7, 1):
        go(send(x_s.at[d], x_r.at[d], x_ss.at[d], x_rs.at[d], x_peer(d)))
    x_r[0] = x_s[0]
    squares = jnp.sum(widened * widened, axis=1, keepdims=True)
    ss_s[...] = jnp.transpose(jnp.broadcast_to(squares, (128, 128)))[0:8, :]
    squared = [
        send(ss_s, ss_r.at[k], q_ss.at[k], q_rs.at[k], {"tp": to}) for k, to in enumerate((right, left, far))
    ]
    for copy in squared:
        go(copy)
    for copy in squared:
        copy.wait_recv()
    squares = ss_s[0:1, :] + ss_r[0, 0:1, :] + ss_r[1, 0:1, :] + ss_r[2, 0:1, :]
    scale = lax.rsqrt(squares / 2048.0 + EPSILON)
    coarse = scale.astype(bf16).astype(f32)
    line = lax.broadcasted_iota(jnp.int32, (128, 128), 0)
    sheet = cw[...] + jnp.where(line == 4, coarse, 0.0) + jnp.where(line == 5, scale - coarse, 0.0)
    cx_s[...] = nt(place[...], sheet.astype(bf16)).astype(bf16).reshape(cx_s.shape)
    for d in range(1, XC):
        go(send(cx_s.at[d], cx_r.at[d], cx_ss.at[d], cx_rs.at[d], x_peer(d)))
    cx_r[0] = cx_s[0]
    for d in range(1, XC):
        send(x_s.at[d], x_r.at[d], x_ss.at[d], x_rs.at[d], x_peer(d)).wait_recv()
    z_s[...] = swapped(x_r[...])
    for d in (1, 7, 2, 6, 3, 5, 4):
        go(send(z_s.at[d], xg.at[0, d], z_ss.at[d], z_rs.at[d], z_peer(d)))
    xg[0, 0] = z_s[0]
    for d in range(1, XC):
        send(cx_s.at[d], cx_r.at[d], cx_ss.at[d], cx_rs.at[d], x_peer(d)).wait_recv()
    cz_s[...] = swapped(cx_r[...])
    for d in range(1, Z):
        go(send(cz_s.at[d], cz_r.at[d], cz_ss.at[d], cz_rs.at[d], z_peer(d)))
    cz_r[0] = cz_s[0]

    order = (0, 1, 7, 2, 6, 3, 5, 4)

    def gather_right(d):
        return send(xg.at[0, d], xg.at[1, d], gr_ss.at[d], gr_rs.at[d], {"tp": right})

    def gather_left(d):
        return send(xg.at[0, d], xg.at[3, d], gl_ss.at[d], gl_rs.at[d], {"tp": left})

    def gather_far(n):
        d = order[n]
        if n % 2 == 0:
            return send(xg.at[1, d], xg.at[2, d], gf_ss.at[d], gf_rs.at[d], {"tp": right})
        return send(xg.at[3, d], xg.at[2, d], gf_ss.at[d], gf_rs.at[d], {"tp": left})

    def pass_on(n):
        if n % 2 == 0:
            gather_right(order[n]).wait_recv()
        else:
            gather_left(order[n]).wait_recv()
        go(gather_far(n))

    for n, d in enumerate(order):
        if d:
            send(z_s.at[d], xg.at[0, d], z_ss.at[d], z_rs.at[d], z_peer(d)).wait_recv()
        go(gather_right(d))
        go(gather_left(d))
        if n >= 5:
            pass_on(n - 5)
    for n in range(3, 8):
        pass_on(n)
    for d in range(1, Z):
        send(cz_s.at[d], cz_r.at[d], cz_ss.at[d], cz_rs.at[d], z_peer(d)).wait_recv()
    for copy in weights:
        copy.wait()
    for n, d in enumerate(order):
        if n % 2 == 0:
            gather_left(d).wait_recv()
        else:
            gather_right(d).wait_recv()
        gather_far(n).wait_recv()

    rows_of = (tp, left, far, right)
    scale = cz_r[...].reshape(256, 128).astype(f32)
    norm = scale[:, 4:5] + scale[:, 5:6]
    for e in range(EPG):
        both = jnp.zeros((256, 256), f32)
        for k in range(4):
            rows = pl.ds(pl.multiple_of(rows_of[k] * 512, 512), 512)
            both = both + nn(
                xg[k].reshape(256, 512), jnp.concatenate([gate[e, rows, :], up[e, rows, :]], axis=1)
            )
        both = both * norm
        g = both[:, 0:128]
        active = g / (1.0 + jnp.exp(-g)) * both[:, 128:256] * scale[:, e : e + 1]
        hidden[:, e * 128 : (e + 1) * 128] = active.astype(bf16)

    def expert_out(q):
        return nn(hidden[...], down[:, :, columns(q)].reshape(512, 512)).astype(bf16).reshape(8, 32, 512)

    back = (4, 3, 5, 2, 6, 1, 7, 0)

    def m_far(n):
        to = right if n % 2 == 0 else left
        d = back[n]
        return send(part.at[2, d], mfar.at[d], mf_ss.at[d], mf_rs.at[d], {"tp": to})

    def m_plain(n):
        d = back[n]
        if n % 2 == 0:
            return send(part.at[3, d], mr.at[d], mp_ss.at[d], mp_rs.at[d], {"tp": left})
        return send(part.at[1, d], ml.at[d], mp_ss.at[d], mp_rs.at[d], {"tp": right})

    def m_comb(n):
        d = back[n]
        if n % 2 == 0:
            return send(mcomb.at[d], ml.at[d], mc_ss.at[d], mc_rs.at[d], {"tp": right})
        return send(mcomb.at[d], mr.at[d], mc_ss.at[d], mc_rs.at[d], {"tp": left})

    def z_back(d):
        return send(rz_s.at[d], rz_r.at[d], rz_ss.at[d], rz_rs.at[d], z_peer(Z - d))

    def x_back(d):
        return send(rx_s.at[d], rx_r.at[d], rx_ss.at[d], rx_rs.at[d], x_peer(XC - d))

    part[2] = expert_out(far)
    for n in range(8):
        go(m_far(n))
    part[1] = expert_out(right)
    part[3] = expert_out(left)
    for n in range(8):
        go(m_plain(n))
    part[0] = expert_out(tp)

    def combine_on(n):
        d = back[n]
        m_far(n).wait_recv()
        mcomb[d] = (mfar[d].astype(f32) + part[1 if n % 2 == 0 else 3, d].astype(f32)).astype(bf16)
        go(m_comb(n))

    def finish_chunk(n):
        d = back[n]
        m_plain(n).wait_recv()
        m_comb(n).wait_recv()
        total = (part[0, d].astype(f32) + ml[d].astype(f32) + mr[d].astype(f32)).astype(bf16)
        if d:
            rz_s[d] = total
            go(z_back(d))
        else:
            rz_r[0] = total

    for n in range(8):
        combine_on(n)
        if n >= 5:
            finish_chunk(n - 5)
    for n in range(3, 8):
        finish_chunk(n)
    for d in range(1, Z):
        z_back(d).wait_recv()
    rx_s[...] = swapped(rz_r[...])
    for d in (4, 3, 5, 2, 6, 7, 1):
        go(x_back(d))
    rx_r[0] = rx_s[0]
    for d in range(1, XC):
        x_back(d).wait_recv()
    moe_ref[...] = lax.dot_general(
        place[...], rx_r[...].reshape(256, 512), (((0,), (0,)), ((), ())), preferred_element_type=f32
    ).astype(bf16)


def routing(route_ref, pair_ref, group_ref, prob_ref, place, cw):
    sp = lax.axis_index("sp")
    f32 = jnp.float32
    line = lax.broadcasted_iota(jnp.int32, (128, 128), 0)
    lane = lax.broadcasted_iota(jnp.int32, (128, 128), 1)
    route = route_ref[...]
    across = jnp.broadcast_to(route, (128, 128))
    down = jnp.transpose(across.astype(f32)).astype(jnp.int32)
    earlier = jnp.where(down == across, 1.0, 0.0) * jnp.where(line < lane, 1.0, 0.0)
    rank = jnp.sum(earlier, axis=0, keepdims=True).astype(jnp.int32)
    dz = ((route >> 3) - sp // XC) & 7
    dx = ((route & 7) - lax.rem(sp, XC)) & 7
    slot = dx * 32 + dz * 4 + rank
    rows = lax.broadcasted_iota(jnp.int32, (256, 128), 0)
    place[...] = jnp.where(rows == slot, 1.0, 0.0).astype(jnp.bfloat16)
    both = prob_ref[0:1, :] + prob_ref[1:2, :]
    sheet = jnp.zeros((128, 128), f32)
    for k in range(2):
        share = group_ref[...] * prob_ref[k : k + 1, :] / both
        sheet = sheet + jnp.where(line == pair_ref[k : k + 1, :], share, 0.0)
    cw[...] = sheet.astype(jnp.bfloat16).astype(f32)


def layer_kernel(
    qw_ref, qn_ref, latent_ref, rope_ref, lgain_ref, cos_ref, sin_ref, route_ref, pair_ref, group_ref, prob_ref, gain_ref,
    wbk_hbm, wbv_hbm, wsk_hbm, wsv_hbm, ow_hbm, on_hbm, resid_hbm, gate_hbm, up_hbm, down_hbm,
    stream_ref, moe_ref,
    wbk, wbv, wsk, wsv, ow, on, resid, gate, up, down, place, cw, att, w_sem, *scratch
):
    sp = lax.axis_index("sp")
    tp = lax.axis_index("tp")
    z = sp // XC
    xc = lax.rem(sp, XC)
    mine = resid_hbm.at[:, pl.ds(pl.multiple_of(tp * 512, 512), 512)]
    pairs = (
        (wbk_hbm, wbk), (wbv_hbm, wbv), (wsk_hbm, wsk), (wsv_hbm, wsv), (ow_hbm, ow), (on_hbm, on), (mine, resid),
        (gate_hbm, gate), (up_hbm, up), (down_hbm, down),
    )
    local = [pltpu.make_async_copy(src, dst, w_sem.at[k]) for k, (src, dst) in enumerate(pairs)]
    barrier = pltpu.get_barrier_semaphore()
    for d in range(1, XC):
        pl.semaphore_signal(
            barrier, inc=1, device_id={"sp": z * XC + lax.rem(xc + d, XC)}, device_id_type=MESH
        )
        pl.semaphore_signal(
            barrier, inc=1, device_id={"sp": lax.rem(z + d, Z) * XC + xc}, device_id_type=MESH
        )
    for d in range(1, 4):
        pl.semaphore_signal(barrier, inc=1, device_id={"tp": lax.rem(tp + d, 4)}, device_id_type=MESH)
    for copy in local:
        copy.start()

    def entered():
        pl.semaphore_wait(barrier, 2 * (XC - 1) + 3)

    sent = []

    def go(copy):
        copy.start()
        sent.append(copy)
        return copy

    attention_part(
        go, entered, local[0:4],
        qw_ref, qn_ref, latent_ref, rope_ref, lgain_ref, wbk, wbv, wsk, wsv, cos_ref, sin_ref, att, *scratch[:A_COUNT]
    )
    routing(route_ref, pair_ref, group_ref, prob_ref, place, cw)
    tail_part(
        go, local[4:7], local[7:10], att, ow, on, resid, gain_ref, place, cw, gate, up, down, stream_ref, moe_ref,
        *scratch[A_COUNT:]
    )
    for copy in sent:
        copy.wait_send()


def layer(vectors, matrices):
    vmem = pl.BlockSpec(memory_space=pltpu.VMEM)
    hbm = pl.BlockSpec(memory_space=pl.ANY)
    bf16, f32, dma = jnp.bfloat16, jnp.float32, pltpu.SemaphoreType.DMA

    def results(*lead, rows=384):
        return [pltpu.VMEM((*lead, rows, BLOCK), bf16), pltpu.VMEM((*lead, 8, BLOCK), f32)]

    def chunks(width, *lead):
        return pltpu.VMEM((*lead, 8, 32, width), bf16)

    half = pltpu.VMEM((2, 64, 512), bf16)
    attention_scratch = [
        pltpu.VMEM((XC, BLOCK, 640), bf16),
        pltpu.VMEM((Z, 64, 1152), bf16),
        pltpu.VMEM((Z, BLOCK, 768), bf16),
        pltpu.VMEM((Z, 384, BLOCK), bf16),
        pltpu.VMEM((4, 384, 256), f32),
        pltpu.VMEM((4, 8, 256), f32),
        pltpu.VMEM((4, 8, 256), f32),
        *results(4), *results(4), *results(4),
        *results(2, rows=192), *results(2, rows=192), *results(2, rows=192), *results(2, rows=192),
        pltpu.VMEM((384, BLOCK), f32),
        dma((6,)), dma((6,)), dma((4, 2)), dma((4, 2)), dma((5, 2)), dma((5, 2)), dma((4, 2)), dma((4, 2)),
        dma((4,)), dma((4,)), dma((4,)), dma((4,)), dma((6,)), dma((6,)), dma((6,)), dma((6,)),
    ]
    assert len(attention_scratch) == A_COUNT
    return pl.pallas_call(
        layer_kernel,
        out_shape=[jax.ShapeDtypeStruct((BLOCK, 512), bf16)] * 2,
        in_specs=[vmem] * 12 + [hbm] * 10,
        out_specs=[vmem] * 2,
        scratch_shapes=[
            *[pltpu.VMEM(m.shape, bf16) for m in matrices[0:6]],
            pltpu.VMEM((BLOCK, 512), bf16),
            *[pltpu.VMEM(m.shape, bf16) for m in matrices[7:10]],
            pltpu.VMEM((256, 128), bf16), pltpu.VMEM((128, 128), f32), pltpu.VMEM((BLOCK, 384), bf16), dma((10,)),
            *attention_scratch,
            pltpu.VMEM((128, 512), f32),
            half, half, pltpu.VMEM((2, 2, 64, 512), bf16), half, half, half,
            pltpu.VMEM((8, 128), f32), pltpu.VMEM((3, 8, 128), f32),
            chunks(128), chunks(128), chunks(128), chunks(128),
            chunks(512), chunks(512), chunks(512), chunks(512, 4), pltpu.VMEM((256, 512), bf16), chunks(512, 4),
            chunks(512), chunks(512), chunks(512), chunks(512), chunks(512), chunks(512), chunks(512), chunks(512),
            dma((6,)), dma((6,)), dma((3,)), dma((3,)),
            *[dma((8,))] * 24,
        ],
        compiler_params=pltpu.CompilerParams(
            collective_id=0, has_side_effects=True, vmem_limit_bytes=60 * 1024 * 1024
        ),
        name="layer",
    )(*vectors, *matrices)


def turn_tables(position):
    lane = jnp.arange(128, dtype=jnp.int32)
    frequency = 1.0 / ROPE_BASE ** ((lane % 32).astype(jnp.float32) * 2.0 / ROPE)
    angle = position.astype(jnp.float32)[:, None] * frequency[None, :]
    sign = jnp.where(lane % 64 < 32, -1.0, 1.0)
    return jnp.cos(angle), jnp.sin(angle) * sign[None, :]


def body(
    query_wide,
    query_narrow,
    latent,
    rope_key,
    latent_norm_weight,
    broad_key_lift,
    broad_value_lift,
    slim_key_lift,
    slim_value_lift,
    out_wide,
    out_narrow,
    resid,
    ffn_gain,
    group_route,
    expert_pair,
    group_prob,
    expert_prob,
    gate_weight,
    up_weight,
    down_weight,
):
    cos, sin = turn_tables(lax.axis_index("sp") * BLOCK + jnp.arange(BLOCK, dtype=jnp.int32))
    stream, moe = layer(
        (
            query_wide, query_narrow, latent, rope_key.T, latent_norm_weight[None, :], cos, sin,
            group_route[None, :], expert_pair.T, group_prob[None, :], expert_prob.T, ffn_gain[None, :],
        ),
        (
            broad_key_lift, broad_value_lift, slim_key_lift, slim_value_lift, out_wide, out_narrow, resid,
            gate_weight[0], up_weight[0], down_weight[0],
        ),
    )
    return (stream.astype(jnp.float32) + moe.astype(jnp.float32)).astype(jnp.bfloat16)


def solution(mesh):
    placed = (
        P("sp", "tp"),
        P("sp", "tp"),
        P("sp", None),
        P("sp", None),
        P(),
        P(None, "tp"),
        P(None, "tp"),
        P(None, "tp"),
        P(None, "tp"),
        P("tp", None),
        P("tp", None),
        P("sp", None),
        P(),
        P("sp"),
        P("sp", None),
        P("sp"),
        P("sp", None),
        P("sp", None, None, "tp"),
        P("sp", None, None, "tp"),
        P("sp", None, "tp", None),
    )
    return jax.shard_map(body, mesh=mesh, in_specs=placed, out_specs=P("sp", "tp"), check_vma=False)
```

```python
import functools

import jax
import jax.numpy as jnp
from jax import lax
from jax.experimental import pallas as pl
from jax.experimental.pallas import tpu as pltpu
from jax.sharding import PartitionSpec as P

PLAIN_WIDTH_WIDE = 128
PLAIN_WIDTH_SLIM = 64
ROPE = 64
VALUE_WIDTH_WIDE = 128
VALUE_WIDTH_SLIM = 64
EPG = 4


ROPE_BASE = 10000.0
EPSILON = 1e-06
MASKED = -1e30


MESH = pl.DeviceIdType.MESH
LOG2E = 1.4426950408889634
Z = 8
XC = 8
BLOCK = 128
A_COUNT = 40
ROWS = ((0, 128), (128, 192), (192, 320), (320, 384))
QUERY = ((0, 256), (384, 512), (128, 384), (512, 640))
KEY = ((0, 256), (512, 640), (256, 512), (640, 768))
WIDE_SCALE = (PLAIN_WIDTH_WIDE + ROPE) ** -0.5 * LOG2E
SLIM_SCALE = (PLAIN_WIDTH_SLIM + ROPE) ** -0.5 * LOG2E


def nt(a, b):
    return lax.dot_general(a, b, (((1,), (1,)), ((), ())), preferred_element_type=jnp.float32)


def nn(a, b):
    return lax.dot_general(a, b, (((1,), (0,)), ((), ())), preferred_element_type=jnp.float32)


def remote(src, dst, send_sem, recv_sem, sp):
    return pltpu.make_async_remote_copy(
        src_ref=src,
        dst_ref=dst,
        send_sem=send_sem,
        recv_sem=recv_sem,
        device_id={"sp": sp},
        device_id_type=MESH,
    )


def attention_part(
    go, entered, lifts,
    qw_ref, qn_ref, latent_ref, rope_ref, gain_ref, wbk_ref, wbv_ref, wsk_ref, wsv_ref, cos_ref, sin_ref,
    att_ref,
    q_all, lat_all, keys, values, scores, kept, acc, peak, total,
    b_s, bs_s, b_r, bs_r, g, gs, far_r, fars_r, comb, combs, lb, lbs, rb, rbs, own,
    q_ss, q_rs, qs_ss, qs_rs, up_ss, up_rs, dn_ss, dn_rs, b_ss, b_rs, bt_ss, bt_rs, o_ss, o_rs, t_ss, t_rs,
):
    bf16, f32 = jnp.bfloat16, jnp.float32
    sp = lax.axis_index("sp")
    z = sp // XC
    xc = lax.rem(sp, XC)
    x = xc // 2
    core = lax.rem(xc, 2)
    base = z * XC
    sibling = base + xc + 1 - 2 * core
    above = lax.rem(sp + XC, Z * XC)
    below = lax.rem(sp + (Z - 1) * XC, Z * XC)
    right = base + lax.rem(x + 1, 4) * 2 + core
    left = base + lax.rem(x + 3, 4) * 2 + core

    lane = lax.broadcasted_iota(jnp.int32, (BLOCK, 128), 1)
    low = lane < 64
    first = lax.rem(lane, 64) < 32
    cos = cos_ref[...]
    sin = sin_ref[...]

    def turned(v):
        swapped = jnp.where(first, pltpu.roll(v, 96, 1), pltpu.roll(v, 32, 1))
        return v * cos + swapped * sin

    v = latent_ref[...].astype(f32)
    v = (v * lax.rsqrt(jnp.mean(v * v, axis=1, keepdims=True) + EPSILON) * gain_ref[...]).astype(bf16)
    lat_all[z, :, 0:512] = v[0:64]
    lat_all[z, :, 512:1024] = v[64:128]
    rope = rope_ref[...].astype(f32)
    rope = turned(jnp.transpose(jnp.concatenate([rope, rope], axis=0)))
    lat_all[z, :, 1024:1152] = jnp.where(low[0:64], rope[0:64], rope[64:128]).astype(bf16)
    q_all[xc, :, 0:128] = qw_ref[:, 0:128]
    middle = qw_ref[:, 128:256].astype(f32)
    last = qw_ref[:, 256:384].astype(f32)
    q_all[xc, :, 128:256] = (turned(jnp.where(low, middle, last)) * WIDE_SCALE).astype(bf16)
    q_all[xc, :, 256:384] = pltpu.roll(jnp.where(low, last, middle), 64, 1).astype(bf16)
    for k in range(2):
        v = qn_ref[:, k * 128 : (k + 1) * 128].astype(f32)
        q_all[xc, :, 384 + k * 128 : 512 + k * 128] = jnp.where(low, v, turned(v) * SLIM_SCALE).astype(bf16)

    entered()

    def ring(slot, h, ssem, rsem, to):
        part = lat_all.at[slot, pl.ds(h * 32, 32)]
        return remote(part, part, ssem, rsem, to)

    def up_copy(s, h):
        return ring(lax.rem(z - s + 1 + Z, Z), h, up_ss.at[s, h], up_rs.at[s, h], above)

    def dn_copy(s, h):
        return ring(lax.rem(z + s - 1, Z), h, dn_ss.at[s, h], dn_rs.at[s, h], below)

    def up_sends(s):
        return (z - s + 1 >= 0) & (z < Z - 1)

    def up_comes(s):
        return z - s >= 0

    def dn_sends(s):
        return lax.rem(z + s - 1, Z) <= 2

    def dn_comes(s):
        return lax.rem(z + s, Z) <= 2

    def start_part(s, h):
        if s <= 4:

            @pl.when(up_sends(s))
            def _():
                up_copy(s, h).start()

        if s <= 3:

            @pl.when(dn_sends(s))
            def _():
                dn_copy(s, h).start()

    def hand_on(s):
        for h in range(2):

            @pl.when(up_comes(s))
            def _(h=h):
                up_copy(s, h).wait_recv()

            if s <= 3:

                @pl.when(dn_comes(s))
                def _(h=h):
                    dn_copy(s, h).wait_recv()

            start_part(s + 1, h)

    start_part(1, 0)
    start_part(1, 1)

    def q_part(slot, h, ssem, rsem, to):
        part = q_all.at[slot, pl.ds(h * 64, 64)]
        return remote(part, part, ssem, rsem, to)

    def x_slot(d):
        return lax.rem(x + d, 4) * 2 + core

    def q_right(h):
        return q_part(xc, h, q_ss.at[h], q_rs.at[h], right)

    def q_left(h):
        return q_part(xc, h, q_ss.at[2 + h], q_rs.at[2 + h], left)

    def q_on(h):
        if h == 0:
            return q_part(x_slot(3), 0, q_ss.at[4], q_rs.at[4], right)
        return q_part(x_slot(1), 1, q_ss.at[5], q_rs.at[5], left)

    def q_sibling(d, h):
        return q_part(x_slot(d), h, qs_ss.at[d, h], qs_rs.at[d, h], sibling)

    go(q_right(0))
    go(q_left(1))
    go(q_right(1))
    go(q_left(0))
    go(q_sibling(0, 0))
    go(q_sibling(0, 1))

    peak[...] = jnp.full(peak.shape, MASKED, f32)
    total[...] = jnp.zeros(total.shape, f32)
    acc[...] = jnp.zeros(acc.shape, f32)

    def project(slot):
        rows = jnp.concatenate([lat_all[slot, :, 0:512], lat_all[slot, :, 512:1024]], axis=0)
        packed = lat_all[slot, :, 1024:1152].astype(f32)
        other = pltpu.roll(packed, 64, 1)
        top = low[0:64]
        rot = jnp.concatenate([jnp.where(top, packed, other), jnp.where(top, other, packed)], axis=0)
        wide = (nn(rows, wbk_ref[...]) * WIDE_SCALE).astype(bf16)
        keys[slot, :, 0:128] = wide[:, 0:128]
        keys[slot, :, 128:256] = jnp.where(low, rot, 0.0).astype(bf16)
        keys[slot, :, 256:384] = jnp.where(low, 0.0, rot).astype(bf16)
        keys[slot, :, 384:512] = wide[:, 128:256]
        slim = nn(rows, wsk_ref[...]) * SLIM_SCALE
        keys[slot, :, 512:640] = jnp.where(low, slim, rot).astype(bf16)
        keys[slot, :, 640:768] = jnp.where(low, pltpu.roll(slim, 64, 1), rot).astype(bf16)
        wide = jnp.transpose(nn(rows, wbv_ref[...])).astype(bf16)
        slim = jnp.transpose(nn(rows, wsv_ref[...])).astype(bf16)
        values[slot, 0:128] = wide[0:128]
        values[slot, 128:192] = slim[0:64]
        values[slot, 192:320] = wide[128:256]
        values[slot, 320:384] = slim[64:128]

    def attend(slots, own_block=False):
        units = [(c, h) for c in range(4) for h in range(4)]

        def score(n):
            c, h = units[n]
            ql, qh = QUERY[h]
            kl, kh = KEY[h]
            q = q_all[2 * c : 2 * c + 2, :, ql:qh].reshape(256, qh - ql)
            top = peak[c, h : h + 1, :]
            kept[c, h : h + 1, :] = top
            for b, slot in enumerate(slots):
                s = nt(keys[slot, :, kl:kh], q)
                if own_block:
                    key_pos = xc * BLOCK + lax.broadcasted_iota(jnp.int32, (BLOCK, 256), 0)
                    query_pos = c * 256 + lax.broadcasted_iota(jnp.int32, (BLOCK, 256), 1)
                    s = jnp.where(key_pos <= query_pos, s, MASKED)
                scores[n, b * BLOCK : (b + 1) * BLOCK, :] = s
                top = jnp.maximum(top, jnp.max(s, axis=0, keepdims=True))
            peak[c, h : h + 1, :] = top

        def add(n):
            c, h = units[n]
            lo, hi = ROWS[h]
            top = peak[c, h : h + 1, :]
            keep = jnp.exp2(kept[c, h : h + 1, :] - top)
            weights = jnp.exp2(scores[n, 0 : len(slots) * BLOCK, :] - top)
            total[c, h : h + 1, :] = total[c, h : h + 1, :] * keep + jnp.sum(weights, axis=0, keepdims=True)
            v = jnp.concatenate([values[slot, lo:hi, :] for slot in slots], axis=1)
            acc[c, lo:hi, :] = acc[c, lo:hi, :] * keep + nn(v, weights.astype(bf16))

        ahead = 16
        for n in range(16 + ahead):
            if n < 16:
                score(n)
            if n >= ahead:
                add(n - ahead)

    for copy in lifts:
        copy.wait()
    project(z)
    hand_on(1)
    q_right(0).wait_recv()
    go(q_on(0))
    q_left(1).wait_recv()
    go(q_on(1))
    go(q_sibling(3, 0))
    go(q_sibling(1, 1))
    q_right(1).wait_recv()
    go(q_sibling(3, 1))
    q_left(0).wait_recv()
    go(q_sibling(1, 0))
    hand_on(2)
    for h in range(2):
        q_on(h).wait_recv()
        go(q_sibling(2, h))

    def needed(i):
        s, up = i // 2 + 1, lax.rem(i, 2) == 0
        slot = jnp.where(up, z - s, z + s - Z)
        return slot, (slot >= 0) & (up | (s <= 3))

    def project_some(lo, hi):
        def some(i, carry):
            slot, wanted = needed(i)

            @pl.when(wanted)
            def _():
                project(slot)

            return carry

        lax.fori_loop(lo, hi, some, 0)

    project_some(0, 4)
    for d in (0, 1, 3, 2):
        for h in range(2):
            q_sibling(d, h).wait_recv()
    attend([z], True)

    def visit(s, carry):
        up, dn = z - s, z + s - Z
        both = (up >= 0) & (dn >= 0) & (s <= 3)

        @pl.when(s == 2)
        def _():
            hand_on(3)
            project_some(4, 6)

        @pl.when(s == 4)
        def _():
            hand_on(4)
            project_some(6, 7)

        @pl.when(both)
        def _():
            attend([up, dn])

        @pl.when(jnp.logical_not(both) & ((up >= 0) | ((dn >= 0) & (s <= 3))))
        def _():
            attend([jnp.where(up >= 0, up, dn)])

        return carry

    lax.fori_loop(1, 5, visit, 0)

    def block_of(d, which):
        lanes = pl.ds(pl.multiple_of(which * 128, 128), 128)
        chip = lax.rem(x + d, 4)
        stats = jnp.concatenate([peak[chip, 0:4, lanes], total[chip, 0:4, lanes]], axis=0)
        return [acc[chip, lo:hi, lanes] / stats[4 + h : 5 + h, :] for h, (lo, hi) in enumerate(ROWS)], stats

    def merge(parts, heads=(0, 1, 2, 3)):
        results, tops, wholes = [], [], []
        for h in heads:
            top = functools.reduce(jnp.maximum, [stats[h : h + 1, :] for _, stats in parts])
            shares = [jnp.exp2(stats[h : h + 1, :] - top) * stats[4 + h : 5 + h, :] for _, stats in parts]
            whole = functools.reduce(jnp.add, shares)
            results.append(
                functools.reduce(jnp.add, [rows[h] * (share / whole) for (rows, _), share in zip(parts, shares)])
            )
            tops.append(top)
            wholes.append(whole)
        return results, tops, wholes

    def rows_of(ref):
        return [ref[lo:hi, :].astype(f32) for lo, hi in ROWS]

    def half_rows(ref, h):
        mine = {2 * h: ref[0:128, :].astype(f32), 2 * h + 1: ref[128:192, :].astype(f32)}
        return [mine.get(k) for k in range(4)]

    def b_copy(d):
        return remote(b_s.at[d], b_r.at[lax.rem(d + 0, 4)], b_ss.at[d], b_rs.at[d], sibling)

    def bs_copy(d):
        return remote(bs_s.at[d], bs_r.at[d], bt_ss.at[d], bt_rs.at[d], sibling)

    for d in (2, 1, 3, 0):
        rows, stats = block_of(d, 1 - core)
        bs_s[d] = stats
        for h, (lo, hi) in enumerate(ROWS):
            b_s[d, lo:hi, :] = rows[h].astype(bf16)
        go(bs_copy(d))
        go(b_copy(d))

    def pair(src, ssrc, dst, sdst, k, to):
        return (
            remote(ssrc, sdst, t_ss.at[k], t_rs.at[k], to),
            remote(src, dst, o_ss.at[k], o_rs.at[k], to),
        )

    def half(ref, d, h):
        return ref.at[d, pl.ds(h * 192, 192)]

    hops = [
        pair(half(g, 2, 0), gs.at[2], far_r.at[0], fars_r.at[0], 0, right),
        pair(half(g, 2, 1), gs.at[2], far_r.at[1], fars_r.at[1], 1, left),
        pair(half(g, 1, 1), gs.at[1], lb.at[1], lbs.at[1], 2, right),
        pair(half(g, 3, 0), gs.at[3], rb.at[0], rbs.at[0], 3, left),
        pair(comb.at[0], combs.at[0], lb.at[0], lbs.at[0], 4, right),
        pair(comb.at[1], combs.at[1], rb.at[1], rbs.at[1], 5, left),
    ]

    def start_hop(k):
        for copy in hops[k]:
            go(copy)

    def await_hop(k):
        for copy in hops[k]:
            copy.wait_recv()

    for d in (2, 1, 3, 0):
        bs_copy(d).wait_recv()
        b_copy(d).wait_recv()
        results, tops, wholes = merge([block_of(d, core), (rows_of(b_r.at[d]), bs_r[d])])
        gs[d] = jnp.concatenate(tops + wholes, axis=0)
        for h, (lo, hi) in enumerate(ROWS):
            if d == 0:
                own[lo:hi, :] = results[h]
            else:
                g[d, lo:hi, :] = results[h].astype(bf16)
        if d == 2:
            start_hop(0)
            start_hop(1)
        elif d == 1:
            start_hop(2)
        elif d == 3:
            start_hop(3)
    for h, d in ((0, 1), (1, 3)):
        await_hop(h)
        heads = (2 * h, 2 * h + 1)
        mine = half_rows(g.at[d, pl.ds(h * 192, 192)], h)
        results, tops, wholes = merge([(half_rows(far_r.at[h], h), fars_r[h]), (mine, gs[d])], heads)
        comb[h, 0:128, :] = results[0].astype(bf16)
        comb[h, 128:192, :] = results[1].astype(bf16)
        idle = jnp.zeros((2, 128), f32)
        tops, wholes = jnp.concatenate(tops, axis=0), jnp.concatenate(wholes, axis=0)
        order = [tops, idle, wholes, idle] if h == 0 else [idle, tops, idle, wholes]
        combs[h] = jnp.concatenate(order, axis=0)
        start_hop(4 + h)
    for k in range(2, 6):
        await_hop(k)
    final = []
    for h in range(2):
        mine = [own[lo:hi, :] for lo, hi in ROWS]
        results, _, _ = merge(
            [(mine, gs[0]), (half_rows(lb.at[h], h), lbs[h]), (half_rows(rb.at[h], h), rbs[h])], (2 * h, 2 * h + 1)
        )
        final.append(results)
    att_ref[:, 0:128] = jnp.transpose(final[0][0]).astype(bf16)
    att_ref[:, 128:256] = jnp.transpose(final[1][0]).astype(bf16)
    att_ref[:, 256:384] = jnp.transpose(jnp.concatenate([final[0][1], final[1][1]], axis=0)).astype(bf16)

    for s in range(1, 5):
        for h in range(2):

            @pl.when(up_sends(s))
            def _(s=s, h=h):
                up_copy(s, h).wait_send()

            if s <= 3:

                @pl.when(dn_sends(s))
                def _(s=s, h=h):
                    dn_copy(s, h).wait_send()


def tail_part(
    go, projections, weights,
    att_ref, ow_ref, on_ref, resid, gain_ref, place, cw, gate, up, down, stream_ref, moe_ref,
    own, far_s, far_r, near_s, comb_s, lb, rb, ss_s, ss_r,
    cx_s, cx_r, cz_s, cz_r, x_s, x_r, z_s, xg, hidden, part, mfar, mcomb, ml, mr, rz_s, rz_r, rx_s, rx_r,
    p_ss, p_rs, q_ss, q_rs, cx_ss, cx_rs, cz_ss, cz_rs, x_ss, x_rs, z_ss, z_rs,
    gr_ss, gr_rs, gl_ss, gl_rs, gf_ss, gf_rs, mf_ss, mf_rs, mp_ss, mp_rs, mc_ss, mc_rs,
    rz_ss, rz_rs, rx_ss, rx_rs,
):
    sp = lax.axis_index("sp")
    tp = lax.axis_index("tp")
    z = sp // XC
    xc = lax.rem(sp, XC)
    right, left, far = lax.rem(tp + 1, 4), lax.rem(tp + 3, 4), lax.rem(tp + 2, 4)

    def x_peer(d):
        return {"sp": z * XC + lax.rem(xc + d, XC)}

    def z_peer(d):
        return {"sp": lax.rem(z + d, Z) * XC + xc}

    def send(src, dst, ssem, rsem, to):
        return pltpu.make_async_remote_copy(
            src_ref=src, dst_ref=dst, send_sem=ssem, recv_sem=rsem, device_id=to, device_id_type=MESH
        )

    bf16, f32 = jnp.bfloat16, jnp.float32
    def columns(q):
        return pl.ds(pl.multiple_of(q * 512, 512), 512)

    def quarter(q):
        return nn(att_ref[:, 0:256], ow_ref[:, columns(q)]) + nn(att_ref[:, 256:384], on_ref[:, columns(q)])

    for copy in projections:
        copy.wait()
    far_s[...] = quarter(far).astype(bf16).reshape(far_s.shape)

    go(send(far_s.at[0], far_r.at[0], p_ss.at[0], p_rs.at[0], {"tp": right}))
    go(send(far_s.at[1], far_r.at[1], p_ss.at[1], p_rs.at[1], {"tp": left}))
    near_s[0] = quarter(right).astype(bf16).reshape(2, 64, 512)
    to_right = send(near_s.at[0, 1], lb.at[1], p_ss.at[2], p_rs.at[2], {"tp": right})
    go(to_right)
    near_s[1] = quarter(left).astype(bf16).reshape(2, 64, 512)
    to_left = send(near_s.at[1, 0], rb.at[0], p_ss.at[3], p_rs.at[3], {"tp": left})
    go(to_left)

    row = lax.broadcasted_iota(jnp.int32, (256, 256), 0)
    col = lax.broadcasted_iota(jnp.int32, (256, 256), 1)
    swap = (col == lax.rem(row // 4, 8) * 32 + (row // 32) * 4 + lax.rem(row, 4)).astype(f32).astype(bf16)

    def swapped(block):
        return nn(swap, block.reshape(256, block.shape[-1])).astype(bf16).reshape(block.shape)

    own[...] = quarter(tp)
    far_right = send(far_s.at[0], far_r.at[0], p_ss.at[0], p_rs.at[0], {"tp": right})
    far_right.wait_recv()
    comb_s[0] = (far_r[0].astype(f32) + near_s[0, 0].astype(f32)).astype(bf16)
    comb_right = send(comb_s.at[0], lb.at[0], p_ss.at[4], p_rs.at[4], {"tp": right})
    go(comb_right)
    far_left = send(far_s.at[1], far_r.at[1], p_ss.at[1], p_rs.at[1], {"tp": left})
    far_left.wait_recv()
    comb_s[1] = (far_r[1].astype(f32) + near_s[1, 1].astype(f32)).astype(bf16)
    comb_left = send(comb_s.at[1], rb.at[1], p_ss.at[5], p_rs.at[5], {"tp": left})
    go(comb_left)

    for copy in (to_right, to_left, comb_right, comb_left):
        copy.wait_recv()
    share = lb[...].astype(f32).reshape(128, 512) + rb[...].astype(f32).reshape(128, 512) + own[...]
    rounded = (resid[...].astype(f32) + share).astype(bf16)
    stream_ref[...] = rounded
    widened = rounded.astype(f32)
    scaled = (widened * gain_ref[:, columns(tp)]).astype(bf16)
    x_s[...] = nn(place[...], scaled).astype(bf16).reshape(x_s.shape)
    for d in (4, 3, 5, 2, 6, 7, 1):
        go(send(x_s.at[d], x_r.at[d], x_ss.at[d], x_rs.at[d], x_peer(d)))
    x_r[0] = x_s[0]
    squares = jnp.sum(widened * widened, axis=1, keepdims=True)
    ss_s[...] = jnp.transpose(jnp.broadcast_to(squares, (128, 128)))[0:8, :]
    squared = [
        send(ss_s, ss_r.at[k], q_ss.at[k], q_rs.at[k], {"tp": to}) for k, to in enumerate((right, left, far))
    ]
    for copy in squared:
        go(copy)
    for copy in squared:
        copy.wait_recv()
    squares = ss_s[0:1, :] + ss_r[0, 0:1, :] + ss_r[1, 0:1, :] + ss_r[2, 0:1, :]
    scale = lax.rsqrt(squares / 2048.0 + EPSILON)
    coarse = scale.astype(bf16).astype(f32)
    line = lax.broadcasted_iota(jnp.int32, (128, 128), 0)
    sheet = cw[...] + jnp.where(line == 4, coarse, 0.0) + jnp.where(line == 5, scale - coarse, 0.0)
    cx_s[...] = nt(place[...], sheet.astype(bf16)).astype(bf16).reshape(cx_s.shape)
    for d in range(1, XC):
        go(send(cx_s.at[d], cx_r.at[d], cx_ss.at[d], cx_rs.at[d], x_peer(d)))
    cx_r[0] = cx_s[0]
    for d in range(1, XC):
        send(x_s.at[d], x_r.at[d], x_ss.at[d], x_rs.at[d], x_peer(d)).wait_recv()
    z_s[...] = swapped(x_r[...])
    for d in (1, 7, 2, 6, 3, 5, 4):
        go(send(z_s.at[d], xg.at[0, d], z_ss.at[d], z_rs.at[d], z_peer(d)))
    xg[0, 0] = z_s[0]
    for d in range(1, XC):
        send(cx_s.at[d], cx_r.at[d], cx_ss.at[d], cx_rs.at[d], x_peer(d)).wait_recv()
    cz_s[...] = swapped(cx_r[...])
    for d in range(1, Z):
        go(send(cz_s.at[d], cz_r.at[d], cz_ss.at[d], cz_rs.at[d], z_peer(d)))
    cz_r[0] = cz_s[0]

    order = (0, 1, 7, 2, 6, 3, 5, 4)

    def gather_right(d):
        return send(xg.at[0, d], xg.at[1, d], gr_ss.at[d], gr_rs.at[d], {"tp": right})

    def gather_left(d):
        return send(xg.at[0, d], xg.at[3, d], gl_ss.at[d], gl_rs.at[d], {"tp": left})

    def gather_far(n):
        d = order[n]
        if n % 2 == 0:
            return send(xg.at[1, d], xg.at[2, d], gf_ss.at[d], gf_rs.at[d], {"tp": right})
        return send(xg.at[3, d], xg.at[2, d], gf_ss.at[d], gf_rs.at[d], {"tp": left})

    def pass_on(n):
        if n % 2 == 0:
            gather_right(order[n]).wait_recv()
        else:
            gather_left(order[n]).wait_recv()
        go(gather_far(n))

    for n, d in enumerate(order):
        if d:
            send(z_s.at[d], xg.at[0, d], z_ss.at[d], z_rs.at[d], z_peer(d)).wait_recv()
        go(gather_right(d))
        go(gather_left(d))
        if n >= 5:
            pass_on(n - 5)
    for n in range(3, 8):
        pass_on(n)
    for d in range(1, Z):
        send(cz_s.at[d], cz_r.at[d], cz_ss.at[d], cz_rs.at[d], z_peer(d)).wait_recv()
    for copy in weights:
        copy.wait()
    for n, d in enumerate(order):
        if n % 2 == 0:
            gather_left(d).wait_recv()
        else:
            gather_right(d).wait_recv()
        gather_far(n).wait_recv()

    rows_of = (tp, left, far, right)
    scale = cz_r[...].reshape(256, 128).astype(f32)
    norm = scale[:, 4:5] + scale[:, 5:6]
    for e in range(EPG):
        both = jnp.zeros((256, 256), f32)
        for k in range(4):
            rows = pl.ds(pl.multiple_of(rows_of[k] * 512, 512), 512)
            both = both + nn(
                xg[k].reshape(256, 512), jnp.concatenate([gate[e, rows, :], up[e, rows, :]], axis=1)
            )
        both = both * norm
        g = both[:, 0:128]
        active = g / (1.0 + jnp.exp(-g)) * both[:, 128:256] * scale[:, e : e + 1]
        hidden[:, e * 128 : (e + 1) * 128] = active.astype(bf16)

    def expert_out(q):
        return nn(hidden[...], down[:, :, columns(q)].reshape(512, 512)).astype(bf16).reshape(8, 32, 512)

    back = (4, 3, 5, 2, 6, 1, 7, 0)

    def m_far(n):
        to = right if n % 2 == 0 else left
        d = back[n]
        return send(part.at[2, d], mfar.at[d], mf_ss.at[d], mf_rs.at[d], {"tp": to})

    def m_plain(n):
        d = back[n]
        if n % 2 == 0:
            return send(part.at[3, d], mr.at[d], mp_ss.at[d], mp_rs.at[d], {"tp": left})
        return send(part.at[1, d], ml.at[d], mp_ss.at[d], mp_rs.at[d], {"tp": right})

    def m_comb(n):
        d = back[n]
        if n % 2 == 0:
            return send(mcomb.at[d], ml.at[d], mc_ss.at[d], mc_rs.at[d], {"tp": right})
        return send(mcomb.at[d], mr.at[d], mc_ss.at[d], mc_rs.at[d], {"tp": left})

    def z_back(d):
        return send(rz_s.at[d], rz_r.at[d], rz_ss.at[d], rz_rs.at[d], z_peer(Z - d))

    def x_back(d):
        return send(rx_s.at[d], rx_r.at[d], rx_ss.at[d], rx_rs.at[d], x_peer(XC - d))

    part[2] = expert_out(far)
    for n in range(8):
        go(m_far(n))
    part[1] = expert_out(right)
    part[3] = expert_out(left)
    for n in range(8):
        go(m_plain(n))
    part[0] = expert_out(tp)

    def combine_on(n):
        d = back[n]
        m_far(n).wait_recv()
        mcomb[d] = (mfar[d].astype(f32) + part[1 if n % 2 == 0 else 3, d].astype(f32)).astype(bf16)
        go(m_comb(n))

    def finish_chunk(n):
        d = back[n]
        m_plain(n).wait_recv()
        m_comb(n).wait_recv()
        total = (part[0, d].astype(f32) + ml[d].astype(f32) + mr[d].astype(f32)).astype(bf16)
        if d:
            rz_s[d] = total
            go(z_back(d))
        else:
            rz_r[0] = total

    for n in range(8):
        combine_on(n)
        if n >= 5:
            finish_chunk(n - 5)
    for n in range(3, 8):
        finish_chunk(n)
    for d in range(1, Z):
        z_back(d).wait_recv()
    rx_s[...] = swapped(rz_r[...])
    for d in (4, 3, 5, 2, 6, 7, 1):
        go(x_back(d))
    rx_r[0] = rx_s[0]
    for d in range(1, XC):
        x_back(d).wait_recv()
    moe_ref[...] = lax.dot_general(
        place[...], rx_r[...].reshape(256, 512), (((0,), (0,)), ((), ())), preferred_element_type=f32
    ).astype(bf16)


def routing(route_ref, pair_ref, group_ref, prob_ref, place, cw):
    sp = lax.axis_index("sp")
    f32 = jnp.float32
    line = lax.broadcasted_iota(jnp.int32, (128, 128), 0)
    lane = lax.broadcasted_iota(jnp.int32, (128, 128), 1)
    route = route_ref[...]
    across = jnp.broadcast_to(route, (128, 128))
    down = jnp.transpose(across.astype(f32)).astype(jnp.int32)
    earlier = jnp.where(down == across, 1.0, 0.0) * jnp.where(line < lane, 1.0, 0.0)
    rank = jnp.sum(earlier, axis=0, keepdims=True).astype(jnp.int32)
    dz = ((route >> 3) - sp // XC) & 7
    dx = ((route & 7) - lax.rem(sp, XC)) & 7
    slot = dx * 32 + dz * 4 + rank
    rows = lax.broadcasted_iota(jnp.int32, (256, 128), 0)
    place[...] = jnp.where(rows == slot, 1.0, 0.0).astype(jnp.bfloat16)
    both = prob_ref[0:1, :] + prob_ref[1:2, :]
    sheet = jnp.zeros((128, 128), f32)
    for k in range(2):
        share = group_ref[...] * prob_ref[k : k + 1, :] / both
        sheet = sheet + jnp.where(line == pair_ref[k : k + 1, :], share, 0.0)
    cw[...] = sheet.astype(jnp.bfloat16).astype(f32)


def layer_kernel(
    qw_ref, qn_ref, latent_ref, rope_ref, lgain_ref, cos_ref, sin_ref, route_ref, pair_ref, group_ref, prob_ref, gain_ref,
    wbk_hbm, wbv_hbm, wsk_hbm, wsv_hbm, ow_hbm, on_hbm, resid_hbm, gate_hbm, up_hbm, down_hbm,
    stream_ref, moe_ref,
    wbk, wbv, wsk, wsv, ow, on, resid, gate, up, down, place, cw, att, w_sem, *scratch
):
    sp = lax.axis_index("sp")
    tp = lax.axis_index("tp")
    z = sp // XC
    xc = lax.rem(sp, XC)
    mine = resid_hbm.at[:, pl.ds(pl.multiple_of(tp * 512, 512), 512)]
    pairs = (
        (wbk_hbm, wbk), (wbv_hbm, wbv), (wsk_hbm, wsk), (wsv_hbm, wsv), (ow_hbm, ow), (on_hbm, on), (mine, resid),
        (gate_hbm, gate), (up_hbm, up), (down_hbm, down),
    )
    local = [pltpu.make_async_copy(src, dst, w_sem.at[k]) for k, (src, dst) in enumerate(pairs)]
    barrier = pltpu.get_barrier_semaphore()
    for d in range(1, XC):
        pl.semaphore_signal(
            barrier, inc=1, device_id={"sp": z * XC + lax.rem(xc + d, XC)}, device_id_type=MESH
        )
        pl.semaphore_signal(
            barrier, inc=1, device_id={"sp": lax.rem(z + d, Z) * XC + xc}, device_id_type=MESH
        )
    for d in range(1, 4):
        pl.semaphore_signal(barrier, inc=1, device_id={"tp": lax.rem(tp + d, 4)}, device_id_type=MESH)
    for copy in local:
        copy.start()

    def entered():
        pl.semaphore_wait(barrier, 2 * (XC - 1) + 3)

    sent = []

    def go(copy):
        copy.start()
        sent.append(copy)
        return copy

    attention_part(
        go, entered, local[0:4],
        qw_ref, qn_ref, latent_ref, rope_ref, lgain_ref, wbk, wbv, wsk, wsv, cos_ref, sin_ref, att, *scratch[:A_COUNT]
    )
    routing(route_ref, pair_ref, group_ref, prob_ref, place, cw)
    tail_part(
        go, local[4:7], local[7:10], att, ow, on, resid, gain_ref, place, cw, gate, up, down, stream_ref, moe_ref,
        *scratch[A_COUNT:]
    )
    for copy in sent:
        copy.wait_send()


def layer(vectors, matrices):
    vmem = pl.BlockSpec(memory_space=pltpu.VMEM)
    hbm = pl.BlockSpec(memory_space=pl.ANY)
    bf16, f32, dma = jnp.bfloat16, jnp.float32, pltpu.SemaphoreType.DMA

    def results(*lead, rows=384):
        return [pltpu.VMEM((*lead, rows, BLOCK), bf16), pltpu.VMEM((*lead, 8, BLOCK), f32)]

    def chunks(width, *lead):
        return pltpu.VMEM((*lead, 8, 32, width), bf16)

    half = pltpu.VMEM((2, 64, 512), bf16)
    attention_scratch = [
        pltpu.VMEM((XC, BLOCK, 640), bf16),
        pltpu.VMEM((Z, 64, 1152), bf16),
        pltpu.VMEM((Z, BLOCK, 768), bf16),
        pltpu.VMEM((Z, 384, BLOCK), bf16),
        pltpu.VMEM((16, 2 * BLOCK, 256), f32),
        pltpu.VMEM((4, 8, 256), f32),
        pltpu.VMEM((4, 384, 256), f32),
        pltpu.VMEM((4, 8, 256), f32),
        pltpu.VMEM((4, 8, 256), f32),
        *results(4), *results(4), *results(4),
        *results(2, rows=192), *results(2, rows=192), *results(2, rows=192), *results(2, rows=192),
        pltpu.VMEM((384, BLOCK), f32),
        dma((6,)), dma((6,)), dma((4, 2)), dma((4, 2)), dma((5, 2)), dma((5, 2)), dma((4, 2)), dma((4, 2)),
        dma((4,)), dma((4,)), dma((4,)), dma((4,)), dma((6,)), dma((6,)), dma((6,)), dma((6,)),
    ]
    assert len(attention_scratch) == A_COUNT
    return pl.pallas_call(
        layer_kernel,
        out_shape=[jax.ShapeDtypeStruct((BLOCK, 512), bf16)] * 2,
        in_specs=[vmem] * 12 + [hbm] * 10,
        out_specs=[vmem] * 2,
        scratch_shapes=[
            *[pltpu.VMEM(m.shape, bf16) for m in matrices[0:6]],
            pltpu.VMEM((BLOCK, 512), bf16),
            *[pltpu.VMEM(m.shape, bf16) for m in matrices[7:10]],
            pltpu.VMEM((256, 128), bf16), pltpu.VMEM((128, 128), f32), pltpu.VMEM((BLOCK, 384), bf16), dma((10,)),
            *attention_scratch,
            pltpu.VMEM((128, 512), f32),
            half, half, pltpu.VMEM((2, 2, 64, 512), bf16), half, half, half,
            pltpu.VMEM((8, 128), f32), pltpu.VMEM((3, 8, 128), f32),
            chunks(128), chunks(128), chunks(128), chunks(128),
            chunks(512), chunks(512), chunks(512), chunks(512, 4), pltpu.VMEM((256, 512), bf16), chunks(512, 4),
            chunks(512), chunks(512), chunks(512), chunks(512), chunks(512), chunks(512), chunks(512), chunks(512),
            dma((6,)), dma((6,)), dma((3,)), dma((3,)),
            *[dma((8,))] * 24,
        ],
        compiler_params=pltpu.CompilerParams(
            collective_id=0, has_side_effects=True, vmem_limit_bytes=60 * 1024 * 1024
        ),
        name="layer",
    )(*vectors, *matrices)


def turn_tables(position):
    lane = jnp.arange(128, dtype=jnp.int32)
    frequency = 1.0 / ROPE_BASE ** ((lane % 32).astype(jnp.float32) * 2.0 / ROPE)
    angle = position.astype(jnp.float32)[:, None] * frequency[None, :]
    sign = jnp.where(lane % 64 < 32, -1.0, 1.0)
    return jnp.cos(angle), jnp.sin(angle) * sign[None, :]


def body(
    query_wide,
    query_narrow,
    latent,
    rope_key,
    latent_norm_weight,
    broad_key_lift,
    broad_value_lift,
    slim_key_lift,
    slim_value_lift,
    out_wide,
    out_narrow,
    resid,
    ffn_gain,
    group_route,
    expert_pair,
    group_prob,
    expert_prob,
    gate_weight,
    up_weight,
    down_weight,
):
    cos, sin = turn_tables(lax.axis_index("sp") * BLOCK + jnp.arange(BLOCK, dtype=jnp.int32))
    stream, moe = layer(
        (
            query_wide, query_narrow, latent, rope_key.T, latent_norm_weight[None, :], cos, sin,
            group_route[None, :], expert_pair.T, group_prob[None, :], expert_prob.T, ffn_gain[None, :],
        ),
        (
            broad_key_lift, broad_value_lift, slim_key_lift, slim_value_lift, out_wide, out_narrow, resid,
            gate_weight[0], up_weight[0], down_weight[0],
        ),
    )
    return (stream.astype(jnp.float32) + moe.astype(jnp.float32)).astype(jnp.bfloat16)


def solution(mesh):
    placed = (
        P("sp", "tp"),
        P("sp", "tp"),
        P("sp", None),
        P("sp", None),
        P(),
        P(None, "tp"),
        P(None, "tp"),
        P(None, "tp"),
        P(None, "tp"),
        P("tp", None),
        P("tp", None),
        P("sp", None),
        P(),
        P("sp"),
        P("sp", None),
        P("sp"),
        P("sp", None),
        P("sp", None, None, "tp"),
        P("sp", None, None, "tp"),
        P("sp", None, "tp", None),
    )
    return jax.shard_map(body, mesh=mesh, in_specs=placed, out_specs=P("sp", "tp"), check_vma=False)
```

```python
import functools

import jax
import jax.numpy as jnp
from jax import lax
from jax.experimental import pallas as pl
from jax.experimental.pallas import tpu as pltpu
from jax.sharding import PartitionSpec as P

PLAIN_WIDTH_WIDE = 128
PLAIN_WIDTH_SLIM = 64
ROPE = 64
VALUE_WIDTH_WIDE = 128
VALUE_WIDTH_SLIM = 64
EPG = 4


ROPE_BASE = 10000.0
EPSILON = 1e-06
MASKED = -1e30


MESH = pl.DeviceIdType.MESH
LOG2E = 1.4426950408889634
Z = 8
XC = 8
BLOCK = 128
ORDER = (4, 3, 5, 2, 6, 1, 7, 0)
A_COUNT = 40
ROWS = ((0, 128), (128, 192), (192, 320), (320, 384))
QUERY = ((0, 256), (384, 512), (128, 384), (512, 640))
KEY = ((0, 256), (512, 640), (256, 512), (640, 768))
WIDE_SCALE = (PLAIN_WIDTH_WIDE + ROPE) ** -0.5 * LOG2E
SLIM_SCALE = (PLAIN_WIDTH_SLIM + ROPE) ** -0.5 * LOG2E


def nt(a, b):
    return lax.dot_general(a, b, (((1,), (1,)), ((), ())), preferred_element_type=jnp.float32)


def nn(a, b):
    return lax.dot_general(a, b, (((1,), (0,)), ((), ())), preferred_element_type=jnp.float32)


def remote(src, dst, send_sem, recv_sem, sp):
    return pltpu.make_async_remote_copy(
        src_ref=src,
        dst_ref=dst,
        send_sem=send_sem,
        recv_sem=recv_sem,
        device_id={"sp": sp},
        device_id_type=MESH,
    )


def attention_part(
    go, entered, lifts,
    qw_ref, qn_ref, latent_ref, rope_ref, gain_ref, wbk_ref, wbv_ref, wsk_ref, wsv_ref, cos_ref, sin_ref,
    att_ref,
    q_all, lat_all, keys, values, scores, kept, acc, peak, total,
    b_s, bs_s, b_r, bs_r, g, gs, far_r, fars_r, comb, combs, lb, lbs, rb, rbs, own,
    q_ss, q_rs, qs_ss, qs_rs, up_ss, up_rs, dn_ss, dn_rs, b_ss, b_rs, bt_ss, bt_rs, o_ss, o_rs, t_ss, t_rs,
):
    bf16, f32 = jnp.bfloat16, jnp.float32
    sp = lax.axis_index("sp")
    z = sp // XC
    xc = lax.rem(sp, XC)
    x = xc // 2
    core = lax.rem(xc, 2)
    base = z * XC
    sibling = base + xc + 1 - 2 * core
    above = lax.rem(sp + XC, Z * XC)
    below = lax.rem(sp + (Z - 1) * XC, Z * XC)
    right = base + lax.rem(x + 1, 4) * 2 + core
    left = base + lax.rem(x + 3, 4) * 2 + core

    lane = lax.broadcasted_iota(jnp.int32, (BLOCK, 128), 1)
    low = lane < 64
    first = lax.rem(lane, 64) < 32
    cos = cos_ref[...]
    sin = sin_ref[...]

    def turned(v):
        swapped = jnp.where(first, pltpu.roll(v, 96, 1), pltpu.roll(v, 32, 1))
        return v * cos + swapped * sin

    v = latent_ref[...].astype(f32)
    v = (v * lax.rsqrt(jnp.mean(v * v, axis=1, keepdims=True) + EPSILON) * gain_ref[...]).astype(bf16)
    lat_all[z, :, 0:512] = v[0:64]
    lat_all[z, :, 512:1024] = v[64:128]
    rope = rope_ref[...].astype(f32)
    rope = turned(jnp.transpose(jnp.concatenate([rope, rope], axis=0)))
    lat_all[z, :, 1024:1152] = jnp.where(low[0:64], rope[0:64], rope[64:128]).astype(bf16)
    q_all[xc, :, 0:128] = qw_ref[:, 0:128]
    middle = qw_ref[:, 128:256].astype(f32)
    last = qw_ref[:, 256:384].astype(f32)
    q_all[xc, :, 128:256] = (turned(jnp.where(low, middle, last)) * WIDE_SCALE).astype(bf16)
    q_all[xc, :, 256:384] = pltpu.roll(jnp.where(low, last, middle), 64, 1).astype(bf16)
    for k in range(2):
        v = qn_ref[:, k * 128 : (k + 1) * 128].astype(f32)
        q_all[xc, :, 384 + k * 128 : 512 + k * 128] = jnp.where(low, v, turned(v) * SLIM_SCALE).astype(bf16)

    entered()

    def ring(slot, h, ssem, rsem, to):
        part = lat_all.at[slot, pl.ds(h * 32, 32)]
        return remote(part, part, ssem, rsem, to)

    def up_copy(s, h):
        return ring(lax.rem(z - s + 1 + Z, Z), h, up_ss.at[s, h], up_rs.at[s, h], above)

    def dn_copy(s, h):
        return ring(lax.rem(z + s - 1, Z), h, dn_ss.at[s, h], dn_rs.at[s, h], below)

    def up_sends(s):
        return (z - s + 1 >= 0) & (z < Z - 1)

    def up_comes(s):
        return z - s >= 0

    def dn_sends(s):
        return lax.rem(z + s - 1, Z) <= 2

    def dn_comes(s):
        return lax.rem(z + s, Z) <= 2

    def start_part(s, h):
        if s <= 4:

            @pl.when(up_sends(s))
            def _():
                up_copy(s, h).start()

        if s <= 3:

            @pl.when(dn_sends(s))
            def _():
                dn_copy(s, h).start()

    def hand_on(s):
        for h in range(2):

            @pl.when(up_comes(s))
            def _(h=h):
                up_copy(s, h).wait_recv()

            if s <= 3:

                @pl.when(dn_comes(s))
                def _(h=h):
                    dn_copy(s, h).wait_recv()

            start_part(s + 1, h)

    start_part(1, 0)
    start_part(1, 1)

    def q_part(slot, h, ssem, rsem, to):
        part = q_all.at[slot, pl.ds(h * 64, 64)]
        return remote(part, part, ssem, rsem, to)

    def x_slot(d):
        return lax.rem(x + d, 4) * 2 + core

    def q_right(h):
        return q_part(xc, h, q_ss.at[h], q_rs.at[h], right)

    def q_left(h):
        return q_part(xc, h, q_ss.at[2 + h], q_rs.at[2 + h], left)

    def q_on(h):
        if h == 0:
            return q_part(x_slot(3), 0, q_ss.at[4], q_rs.at[4], right)
        return q_part(x_slot(1), 1, q_ss.at[5], q_rs.at[5], left)

    def q_sibling(d, h):
        return q_part(x_slot(d), h, qs_ss.at[d, h], qs_rs.at[d, h], sibling)

    go(q_right(0))
    go(q_left(1))
    go(q_right(1))
    go(q_left(0))
    go(q_sibling(0, 0))
    go(q_sibling(0, 1))

    peak[...] = jnp.full(peak.shape, MASKED, f32)
    total[...] = jnp.zeros(total.shape, f32)
    acc[...] = jnp.zeros(acc.shape, f32)

    def project(slot):
        rows = jnp.concatenate([lat_all[slot, :, 0:512], lat_all[slot, :, 512:1024]], axis=0)
        packed = lat_all[slot, :, 1024:1152].astype(f32)
        other = pltpu.roll(packed, 64, 1)
        top = low[0:64]
        rot = jnp.concatenate([jnp.where(top, packed, other), jnp.where(top, other, packed)], axis=0)
        wide = (nn(rows, wbk_ref[...]) * WIDE_SCALE).astype(bf16)
        keys[slot, :, 0:128] = wide[:, 0:128]
        keys[slot, :, 128:256] = jnp.where(low, rot, 0.0).astype(bf16)
        keys[slot, :, 256:384] = jnp.where(low, 0.0, rot).astype(bf16)
        keys[slot, :, 384:512] = wide[:, 128:256]
        slim = nn(rows, wsk_ref[...]) * SLIM_SCALE
        keys[slot, :, 512:640] = jnp.where(low, slim, rot).astype(bf16)
        keys[slot, :, 640:768] = jnp.where(low, pltpu.roll(slim, 64, 1), rot).astype(bf16)
        wide = jnp.transpose(nn(rows, wbv_ref[...])).astype(bf16)
        slim = jnp.transpose(nn(rows, wsv_ref[...])).astype(bf16)
        values[slot, 0:128] = wide[0:128]
        values[slot, 128:192] = slim[0:64]
        values[slot, 192:320] = wide[128:256]
        values[slot, 320:384] = slim[64:128]

    def attend(slots, own_block=False):
        units = [(c, h) for c in range(4) for h in range(4)]

        def score(n):
            c, h = units[n]
            ql, qh = QUERY[h]
            kl, kh = KEY[h]
            q = q_all[2 * c : 2 * c + 2, :, ql:qh].reshape(256, qh - ql)
            top = peak[c, h : h + 1, :]
            kept[c, h : h + 1, :] = top
            for b, slot in enumerate(slots):
                s = nt(keys[slot, :, kl:kh], q)
                if own_block:
                    key_pos = xc * BLOCK + lax.broadcasted_iota(jnp.int32, (BLOCK, 256), 0)
                    query_pos = c * 256 + lax.broadcasted_iota(jnp.int32, (BLOCK, 256), 1)
                    s = jnp.where(key_pos <= query_pos, s, MASKED)
                scores[n, b * BLOCK : (b + 1) * BLOCK, :] = s
                top = jnp.maximum(top, jnp.max(s, axis=0, keepdims=True))
            peak[c, h : h + 1, :] = top

        def add(n):
            c, h = units[n]
            lo, hi = ROWS[h]
            top = peak[c, h : h + 1, :]
            keep = jnp.exp2(kept[c, h : h + 1, :] - top)
            weights = jnp.exp2(scores[n, 0 : len(slots) * BLOCK, :] - top)
            total[c, h : h + 1, :] = total[c, h : h + 1, :] * keep + jnp.sum(weights, axis=0, keepdims=True)
            v = jnp.concatenate([values[slot, lo:hi, :] for slot in slots], axis=1)
            acc[c, lo:hi, :] = acc[c, lo:hi, :] * keep + nn(v, weights.astype(bf16))

        ahead = 16
        for n in range(16 + ahead):
            if n < 16:
                score(n)
            if n >= ahead:
                add(n - ahead)

    for copy in lifts:
        copy.wait()
    project(z)
    hand_on(1)
    q_right(0).wait_recv()
    go(q_on(0))
    q_left(1).wait_recv()
    go(q_on(1))
    go(q_sibling(3, 0))
    go(q_sibling(1, 1))
    q_right(1).wait_recv()
    go(q_sibling(3, 1))
    q_left(0).wait_recv()
    go(q_sibling(1, 0))
    hand_on(2)
    for h in range(2):
        q_on(h).wait_recv()
        go(q_sibling(2, h))

    def needed(i):
        s, up = i // 2 + 1, lax.rem(i, 2) == 0
        slot = jnp.where(up, z - s, z + s - Z)
        return slot, (slot >= 0) & (up | (s <= 3))

    def project_some(lo, hi):
        def some(i, carry):
            slot, wanted = needed(i)

            @pl.when(wanted)
            def _():
                project(slot)

            return carry

        lax.fori_loop(lo, hi, some, 0)

    project_some(0, 4)
    for d in (0, 1, 3, 2):
        for h in range(2):
            q_sibling(d, h).wait_recv()
    attend([z], True)

    def visit(s, carry):
        up, dn = z - s, z + s - Z
        both = (up >= 0) & (dn >= 0) & (s <= 3)

        @pl.when(s == 2)
        def _():
            hand_on(3)
            project_some(4, 6)

        @pl.when(s == 4)
        def _():
            hand_on(4)
            project_some(6, 7)

        @pl.when(both)
        def _():
            attend([up, dn])

        @pl.when(jnp.logical_not(both) & ((up >= 0) | ((dn >= 0) & (s <= 3))))
        def _():
            attend([jnp.where(up >= 0, up, dn)])

        return carry

    lax.fori_loop(1, 5, visit, 0)

    def block_of(d, which):
        lanes = pl.ds(pl.multiple_of(which * 128, 128), 128)
        chip = lax.rem(x + d, 4)
        stats = jnp.concatenate([peak[chip, 0:4, lanes], total[chip, 0:4, lanes]], axis=0)
        return [acc[chip, lo:hi, lanes] / stats[4 + h : 5 + h, :] for h, (lo, hi) in enumerate(ROWS)], stats

    def merge(parts, heads=(0, 1, 2, 3)):
        results, tops, wholes = [], [], []
        for h in heads:
            top = functools.reduce(jnp.maximum, [stats[h : h + 1, :] for _, stats in parts])
            shares = [jnp.exp2(stats[h : h + 1, :] - top) * stats[4 + h : 5 + h, :] for _, stats in parts]
            whole = functools.reduce(jnp.add, shares)
            results.append(
                functools.reduce(jnp.add, [rows[h] * (share / whole) for (rows, _), share in zip(parts, shares)])
            )
            tops.append(top)
            wholes.append(whole)
        return results, tops, wholes

    def rows_of(ref):
        return [ref[lo:hi, :].astype(f32) for lo, hi in ROWS]

    def half_rows(ref, h):
        mine = {2 * h: ref[0:128, :].astype(f32), 2 * h + 1: ref[128:192, :].astype(f32)}
        return [mine.get(k) for k in range(4)]

    def b_copy(d):
        return remote(b_s.at[d], b_r.at[lax.rem(d + 0, 4)], b_ss.at[d], b_rs.at[d], sibling)

    def bs_copy(d):
        return remote(bs_s.at[d], bs_r.at[d], bt_ss.at[d], bt_rs.at[d], sibling)

    for d in (2, 1, 3, 0):
        rows, stats = block_of(d, 1 - core)
        bs_s[d] = stats
        for h, (lo, hi) in enumerate(ROWS):
            b_s[d, lo:hi, :] = rows[h].astype(bf16)
        go(bs_copy(d))
        go(b_copy(d))

    def pair(src, ssrc, dst, sdst, k, to):
        return (
            remote(ssrc, sdst, t_ss.at[k], t_rs.at[k], to),
            remote(src, dst, o_ss.at[k], o_rs.at[k], to),
        )

    def half(ref, d, h):
        return ref.at[d, pl.ds(h * 192, 192)]

    hops = [
        pair(half(g, 2, 0), gs.at[2], far_r.at[0], fars_r.at[0], 0, right),
        pair(half(g, 2, 1), gs.at[2], far_r.at[1], fars_r.at[1], 1, left),
        pair(half(g, 1, 1), gs.at[1], lb.at[1], lbs.at[1], 2, right),
        pair(half(g, 3, 0), gs.at[3], rb.at[0], rbs.at[0], 3, left),
        pair(comb.at[0], combs.at[0], lb.at[0], lbs.at[0], 4, right),
        pair(comb.at[1], combs.at[1], rb.at[1], rbs.at[1], 5, left),
    ]

    def start_hop(k):
        for copy in hops[k]:
            go(copy)

    def await_hop(k):
        for copy in hops[k]:
            copy.wait_recv()

    for d in (2, 1, 3, 0):
        bs_copy(d).wait_recv()
        b_copy(d).wait_recv()
        results, tops, wholes = merge([block_of(d, core), (rows_of(b_r.at[d]), bs_r[d])])
        gs[d] = jnp.concatenate(tops + wholes, axis=0)
        for h, (lo, hi) in enumerate(ROWS):
            if d == 0:
                own[lo:hi, :] = results[h]
            else:
                g[d, lo:hi, :] = results[h].astype(bf16)
        if d == 2:
            start_hop(0)
            start_hop(1)
        elif d == 1:
            start_hop(2)
        elif d == 3:
            start_hop(3)
    for h, d in ((0, 1), (1, 3)):
        await_hop(h)
        heads = (2 * h, 2 * h + 1)
        mine = half_rows(g.at[d, pl.ds(h * 192, 192)], h)
        results, tops, wholes = merge([(half_rows(far_r.at[h], h), fars_r[h]), (mine, gs[d])], heads)
        comb[h, 0:128, :] = results[0].astype(bf16)
        comb[h, 128:192, :] = results[1].astype(bf16)
        idle = jnp.zeros((2, 128), f32)
        tops, wholes = jnp.concatenate(tops, axis=0), jnp.concatenate(wholes, axis=0)
        order = [tops, idle, wholes, idle] if h == 0 else [idle, tops, idle, wholes]
        combs[h] = jnp.concatenate(order, axis=0)
        start_hop(4 + h)
    for k in range(2, 6):
        await_hop(k)
    final = []
    for h in range(2):
        mine = [own[lo:hi, :] for lo, hi in ROWS]
        results, _, _ = merge(
            [(mine, gs[0]), (half_rows(lb.at[h], h), lbs[h]), (half_rows(rb.at[h], h), rbs[h])], (2 * h, 2 * h + 1)
        )
        final.append(results)
    att_ref[:, 0:128] = jnp.transpose(final[0][0]).astype(bf16)
    att_ref[:, 128:256] = jnp.transpose(final[1][0]).astype(bf16)
    att_ref[:, 256:384] = jnp.transpose(jnp.concatenate([final[0][1], final[1][1]], axis=0)).astype(bf16)

    for s in range(1, 5):
        for h in range(2):

            @pl.when(up_sends(s))
            def _(s=s, h=h):
                up_copy(s, h).wait_send()

            if s <= 3:

                @pl.when(dn_sends(s))
                def _(s=s, h=h):
                    dn_copy(s, h).wait_send()


def tail_part(
    go, projections, weights,
    att_ref, ow_ref, on_ref, resid, gain_ref, place, cw, gate, up, down, stream_ref, moe_ref,
    own, far_s, far_r, near_s, comb_s, lb, rb, ss_s, ss_r,
    cx_s, cx_r, cz_s, cz_r, x_s, x_r, z_s, xg, hidden, part, mfar, mcomb, ml, mr, rz_s, rz_r, rx_s, rx_r,
    p_ss, p_rs, q_ss, q_rs, cx_ss, cx_rs, cz_ss, cz_rs, x_ss, x_rs, z_ss, z_rs,
    gr_ss, gr_rs, gl_ss, gl_rs, gf_ss, gf_rs, mf_ss, mf_rs, mp_ss, mp_rs, mc_ss, mc_rs,
    rz_ss, rz_rs, rx_ss, rx_rs,
):
    sp = lax.axis_index("sp")
    tp = lax.axis_index("tp")
    z = sp // XC
    xc = lax.rem(sp, XC)
    right, left, far = lax.rem(tp + 1, 4), lax.rem(tp + 3, 4), lax.rem(tp + 2, 4)

    def x_peer(d):
        return {"sp": z * XC + lax.rem(xc + d, XC)}

    def z_peer(d):
        return {"sp": lax.rem(z + d, Z) * XC + xc}

    def send(src, dst, ssem, rsem, to):
        return pltpu.make_async_remote_copy(
            src_ref=src, dst_ref=dst, send_sem=ssem, recv_sem=rsem, device_id=to, device_id_type=MESH
        )

    bf16, f32 = jnp.bfloat16, jnp.float32
    def columns(q):
        return pl.ds(pl.multiple_of(q * 512, 512), 512)

    def quarter(q):
        return nn(att_ref[:, 0:256], ow_ref[:, columns(q)]) + nn(att_ref[:, 256:384], on_ref[:, columns(q)])

    for copy in projections:
        copy.wait()
    far_s[...] = quarter(far).astype(bf16).reshape(far_s.shape)

    go(send(far_s.at[0], far_r.at[0], p_ss.at[0], p_rs.at[0], {"tp": right}))
    go(send(far_s.at[1], far_r.at[1], p_ss.at[1], p_rs.at[1], {"tp": left}))
    near_s[0] = quarter(right).astype(bf16).reshape(2, 64, 512)
    to_right = send(near_s.at[0, 1], lb.at[1], p_ss.at[2], p_rs.at[2], {"tp": right})
    go(to_right)
    near_s[1] = quarter(left).astype(bf16).reshape(2, 64, 512)
    to_left = send(near_s.at[1, 0], rb.at[0], p_ss.at[3], p_rs.at[3], {"tp": left})
    go(to_left)

    row = lax.broadcasted_iota(jnp.int32, (256, 256), 0)
    col = lax.broadcasted_iota(jnp.int32, (256, 256), 1)
    swap = (col == lax.rem(row // 4, 8) * 32 + (row // 32) * 4 + lax.rem(row, 4)).astype(f32).astype(bf16)

    def swapped(block):
        return nn(swap, block.reshape(256, block.shape[-1])).astype(bf16).reshape(block.shape)

    row = lax.broadcasted_iota(jnp.int32, (128, 128), 0)
    col = lax.broadcasted_iota(jnp.int32, (128, 128), 1)
    half_in = (col == lax.rem(row // 4, 8) * 16 + (row // 32) * 4 + lax.rem(row, 4)).astype(f32).astype(bf16)
    half_out = (col == lax.rem(row // 4, 4) * 32 + (row // 16) * 4 + lax.rem(row, 4)).astype(f32).astype(bf16)

    own[...] = quarter(tp)
    far_right = send(far_s.at[0], far_r.at[0], p_ss.at[0], p_rs.at[0], {"tp": right})
    far_right.wait_recv()
    comb_s[0] = (far_r[0].astype(f32) + near_s[0, 0].astype(f32)).astype(bf16)
    comb_right = send(comb_s.at[0], lb.at[0], p_ss.at[4], p_rs.at[4], {"tp": right})
    go(comb_right)
    far_left = send(far_s.at[1], far_r.at[1], p_ss.at[1], p_rs.at[1], {"tp": left})
    far_left.wait_recv()
    comb_s[1] = (far_r[1].astype(f32) + near_s[1, 1].astype(f32)).astype(bf16)
    comb_left = send(comb_s.at[1], rb.at[1], p_ss.at[5], p_rs.at[5], {"tp": left})
    go(comb_left)

    for copy in (to_right, to_left, comb_right, comb_left):
        copy.wait_recv()
    share = lb[...].astype(f32).reshape(128, 512) + rb[...].astype(f32).reshape(128, 512) + own[...]
    rounded = (resid[...].astype(f32) + share).astype(bf16)
    stream_ref[...] = rounded
    widened = rounded.astype(f32)
    scaled = (widened * gain_ref[:, columns(tp)]).astype(bf16)
    x_s[...] = nn(place[...], scaled).astype(bf16).reshape(x_s.shape)
    def x_copy(h, d):
        return send(
            x_s.at[d, pl.ds(h * 16, 16)], x_r.at[h, d], x_ss.at[h, d], x_rs.at[h, d], x_peer(d)
        )

    for h in range(2):
        for d in (4, 3, 5, 2, 6, 7, 1):
            go(x_copy(h, d))
        x_r[h, 0] = x_s[0, h * 16 : (h + 1) * 16]
    squares = jnp.sum(widened * widened, axis=1, keepdims=True)
    ss_s[...] = jnp.transpose(jnp.broadcast_to(squares, (128, 128)))[0:8, :]
    squared = [
        send(ss_s, ss_r.at[k], q_ss.at[k], q_rs.at[k], {"tp": to}) for k, to in enumerate((right, left, far))
    ]
    for copy in squared:
        go(copy)
    for copy in squared:
        copy.wait_recv()
    squares = ss_s[0:1, :] + ss_r[0, 0:1, :] + ss_r[1, 0:1, :] + ss_r[2, 0:1, :]
    scale = lax.rsqrt(squares / 2048.0 + EPSILON)
    coarse = scale.astype(bf16).astype(f32)
    line = lax.broadcasted_iota(jnp.int32, (128, 128), 0)
    sheet = cw[...] + jnp.where(line == 4, coarse, 0.0) + jnp.where(line == 5, scale - coarse, 0.0)
    cx_s[...] = nt(place[...], sheet.astype(bf16)).astype(bf16).reshape(cx_s.shape)
    for d in range(1, XC):
        go(send(cx_s.at[d], cx_r.at[d], cx_ss.at[d], cx_rs.at[d], x_peer(d)))
    cx_r[0] = cx_s[0]
    def z_copy(n):
        return send(z_s.at[n], xg.at[0, n], z_ss.at[n], z_rs.at[n], z_peer(ORDER[n]))

    for h in range(2):
        for d in range(1, XC):
            x_copy(h, d).wait_recv()
        z_s[4 * h : 4 * h + 4] = nn(half_in, x_r[h].reshape(128, 512)).astype(bf16).reshape(4, 32, 512)
        for n in range(4 * h, 4 * h + 4):
            if ORDER[n]:
                go(z_copy(n))
            else:
                xg[0, n] = z_s[n]
    for d in range(1, XC):
        send(cx_s.at[d], cx_r.at[d], cx_ss.at[d], cx_rs.at[d], x_peer(d)).wait_recv()
    cz_s[...] = swapped(cx_r[...])
    def cz_copy(n):
        return send(cz_s.at[n], cz_r.at[n], cz_ss.at[n], cz_rs.at[n], z_peer(ORDER[n]))

    for n in range(7):
        go(cz_copy(n))
    cz_r[7] = cz_s[7]

    def gather_right(n):
        return send(xg.at[0, n], xg.at[1, n], gr_ss.at[n], gr_rs.at[n], {"tp": right})

    def gather_left(n):
        return send(xg.at[0, n], xg.at[3, n], gl_ss.at[n], gl_rs.at[n], {"tp": left})

    def gather_far(n):
        if n % 2 == 0:
            return send(xg.at[1, n], xg.at[2, n], gf_ss.at[n], gf_rs.at[n], {"tp": right})
        return send(xg.at[3, n], xg.at[2, n], gf_ss.at[n], gf_rs.at[n], {"tp": left})

    def pass_on(n):
        if n % 2 == 0:
            gather_right(n).wait_recv()
        else:
            gather_left(n).wait_recv()
        go(gather_far(n))

    arriving = (1, 2, 3, 0, 7, 5, 6, 4)
    for k, n in enumerate(arriving):
        if ORDER[n]:
            z_copy(n).wait_recv()
        go(gather_right(n))
        go(gather_left(n))
        if k >= 5:
            pass_on(arriving[k - 5])
    for k in range(8 - 5, 8):
        pass_on(arriving[k])
    for n in range(7):
        cz_copy(n).wait_recv()
    for copy in weights:
        copy.wait()

    rows_of = (tp, left, far, right)
    scale = cz_r[...].reshape(256, 128).astype(f32)

    def experts(h):
        factors = scale[h * 128 : (h + 1) * 128]
        norm = factors[:, 4:5] + factors[:, 5:6]
        for e in range(EPG):
            both = jnp.zeros((128, 256), f32)
            for k in range(4):
                rows = pl.ds(pl.multiple_of(rows_of[k] * 512, 512), 512)
                both = both + nn(
                    xg[k, 4 * h : 4 * h + 4].reshape(128, 512),
                    jnp.concatenate([gate[e, rows, :], up[e, rows, :]], axis=1),
                )
            both = both * norm
            g = both[:, 0:128]
            active = g / (1.0 + jnp.exp(-g)) * both[:, 128:256] * factors[:, e : e + 1]
            hidden[h * 128 : (h + 1) * 128, e * 128 : (e + 1) * 128] = active.astype(bf16)

    def expert_out(q, h):
        rows = hidden[h * 128 : (h + 1) * 128, :]
        return nn(rows, down[:, :, columns(q)].reshape(512, 512)).astype(bf16).reshape(4, 32, 512)

    def m_far(n):
        to = right if n % 2 == 0 else left
        return send(part.at[2, n], mfar.at[n], mf_ss.at[n], mf_rs.at[n], {"tp": to})

    def m_plain(n):
        if n % 2 == 0:
            return send(part.at[3, n], mr.at[n], mp_ss.at[n], mp_rs.at[n], {"tp": left})
        return send(part.at[1, n], ml.at[n], mp_ss.at[n], mp_rs.at[n], {"tp": right})

    def m_comb(n):
        if n % 2 == 0:
            return send(mcomb.at[n], ml.at[n], mc_ss.at[n], mc_rs.at[n], {"tp": right})
        return send(mcomb.at[n], mr.at[n], mc_ss.at[n], mc_rs.at[n], {"tp": left})

    def z_back(n):
        return send(rz_s.at[n], rz_r.at[n], rz_ss.at[n], rz_rs.at[n], z_peer(Z - ORDER[n]))

    def x_back(h, d):
        return send(
            rx_s.at[h, d], rx_r.at[d, pl.ds(h * 16, 16)], rx_ss.at[h, d], rx_rs.at[h, d], x_peer(XC - d)
        )

    for h in range(2):
        half_of = range(4 * h, 4 * h + 4)
        for n in half_of:
            if n % 2 == 0:
                gather_left(n).wait_recv()
            else:
                gather_right(n).wait_recv()
            gather_far(n).wait_recv()
        experts(h)
        part[2, 4 * h : 4 * h + 4] = expert_out(far, h)
        for n in half_of:
            go(m_far(n))
        part[1, 4 * h : 4 * h + 4] = expert_out(right, h)
        part[3, 4 * h : 4 * h + 4] = expert_out(left, h)
        for n in half_of:
            go(m_plain(n))
        part[0, 4 * h : 4 * h + 4] = expert_out(tp, h)

    def combine_on(n):
        m_far(n).wait_recv()
        mcomb[n] = (mfar[n].astype(f32) + part[1 if n % 2 == 0 else 3, n].astype(f32)).astype(bf16)
        go(m_comb(n))

    def finish_chunk(n):
        m_plain(n).wait_recv()
        m_comb(n).wait_recv()
        total = (part[0, n].astype(f32) + ml[n].astype(f32) + mr[n].astype(f32)).astype(bf16)
        if ORDER[n]:
            rz_s[n] = total
            go(z_back(n))
        else:
            rz_r[n] = total

    for n in range(8):
        combine_on(n)
        if n >= 5:
            finish_chunk(n - 5)
    for n in range(8 - 5, 8):
        finish_chunk(n)
    for h in range(2):
        for n in range(4 * h, 4 * h + 4):
            if ORDER[n]:
                z_back(n).wait_recv()
        rx_s[h] = nn(half_out, rz_r[4 * h : 4 * h + 4].reshape(128, 512)).astype(bf16).reshape(8, 16, 512)
        for d in (4, 3, 5, 2, 6, 7, 1):
            go(x_back(h, d))
        rx_r[0, h * 16 : (h + 1) * 16] = rx_s[h, 0]
    for h in range(2):
        for d in range(1, XC):
            x_back(h, d).wait_recv()
    moe_ref[...] = lax.dot_general(
        place[...], rx_r[...].reshape(256, 512), (((0,), (0,)), ((), ())), preferred_element_type=f32
    ).astype(bf16)


def routing(route_ref, pair_ref, group_ref, prob_ref, place, cw):
    sp = lax.axis_index("sp")
    f32 = jnp.float32
    line = lax.broadcasted_iota(jnp.int32, (128, 128), 0)
    lane = lax.broadcasted_iota(jnp.int32, (128, 128), 1)
    route = route_ref[...]
    across = jnp.broadcast_to(route, (128, 128))
    down = jnp.transpose(across.astype(f32)).astype(jnp.int32)
    earlier = jnp.where(down == across, 1.0, 0.0) * jnp.where(line < lane, 1.0, 0.0)
    rank = jnp.sum(earlier, axis=0, keepdims=True).astype(jnp.int32)
    dz = ((route >> 3) - sp // XC) & 7
    dx = ((route & 7) - lax.rem(sp, XC)) & 7
    place_of = jnp.zeros_like(dz)
    for n, d in enumerate(ORDER):
        place_of = place_of + jnp.where(dz == d, n, 0)
    slot = dx * 32 + place_of * 4 + rank
    rows = lax.broadcasted_iota(jnp.int32, (256, 128), 0)
    place[...] = jnp.where(rows == slot, 1.0, 0.0).astype(jnp.bfloat16)
    both = prob_ref[0:1, :] + prob_ref[1:2, :]
    sheet = jnp.zeros((128, 128), f32)
    for k in range(2):
        share = group_ref[...] * prob_ref[k : k + 1, :] / both
        sheet = sheet + jnp.where(line == pair_ref[k : k + 1, :], share, 0.0)
    cw[...] = sheet.astype(jnp.bfloat16).astype(f32)


def layer_kernel(
    qw_ref, qn_ref, latent_ref, rope_ref, lgain_ref, cos_ref, sin_ref, route_ref, pair_ref, group_ref, prob_ref, gain_ref,
    wbk_hbm, wbv_hbm, wsk_hbm, wsv_hbm, ow_hbm, on_hbm, resid_hbm, gate_hbm, up_hbm, down_hbm,
    stream_ref, moe_ref,
    wbk, wbv, wsk, wsv, ow, on, resid, gate, up, down, place, cw, att, w_sem, *scratch
):
    sp = lax.axis_index("sp")
    tp = lax.axis_index("tp")
    z = sp // XC
    xc = lax.rem(sp, XC)
    mine = resid_hbm.at[:, pl.ds(pl.multiple_of(tp * 512, 512), 512)]
    pairs = (
        (wbk_hbm, wbk), (wbv_hbm, wbv), (wsk_hbm, wsk), (wsv_hbm, wsv), (ow_hbm, ow), (on_hbm, on), (mine, resid),
        (gate_hbm, gate), (up_hbm, up), (down_hbm, down),
    )
    local = [pltpu.make_async_copy(src, dst, w_sem.at[k]) for k, (src, dst) in enumerate(pairs)]
    barrier = pltpu.get_barrier_semaphore()
    for d in range(1, XC):
        pl.semaphore_signal(
            barrier, inc=1, device_id={"sp": z * XC + lax.rem(xc + d, XC)}, device_id_type=MESH
        )
        pl.semaphore_signal(
            barrier, inc=1, device_id={"sp": lax.rem(z + d, Z) * XC + xc}, device_id_type=MESH
        )
    for d in range(1, 4):
        pl.semaphore_signal(barrier, inc=1, device_id={"tp": lax.rem(tp + d, 4)}, device_id_type=MESH)
    for copy in local:
        copy.start()

    def entered():
        pl.semaphore_wait(barrier, 2 * (XC - 1) + 3)

    sent = []

    def go(copy):
        copy.start()
        sent.append(copy)
        return copy

    attention_part(
        go, entered, local[0:4],
        qw_ref, qn_ref, latent_ref, rope_ref, lgain_ref, wbk, wbv, wsk, wsv, cos_ref, sin_ref, att, *scratch[:A_COUNT]
    )
    routing(route_ref, pair_ref, group_ref, prob_ref, place, cw)
    tail_part(
        go, local[4:7], local[7:10], att, ow, on, resid, gain_ref, place, cw, gate, up, down, stream_ref, moe_ref,
        *scratch[A_COUNT:]
    )
    for copy in sent:
        copy.wait_send()


def layer(vectors, matrices):
    vmem = pl.BlockSpec(memory_space=pltpu.VMEM)
    hbm = pl.BlockSpec(memory_space=pl.ANY)
    bf16, f32, dma = jnp.bfloat16, jnp.float32, pltpu.SemaphoreType.DMA

    def results(*lead, rows=384):
        return [pltpu.VMEM((*lead, rows, BLOCK), bf16), pltpu.VMEM((*lead, 8, BLOCK), f32)]

    def chunks(width, *lead):
        return pltpu.VMEM((*lead, 8, 32, width), bf16)

    half = pltpu.VMEM((2, 64, 512), bf16)
    halves = pltpu.VMEM((2, 8, 16, 512), bf16)
    attention_scratch = [
        pltpu.VMEM((XC, BLOCK, 640), bf16),
        pltpu.VMEM((Z, 64, 1152), bf16),
        pltpu.VMEM((Z, BLOCK, 768), bf16),
        pltpu.VMEM((Z, 384, BLOCK), bf16),
        pltpu.VMEM((16, 2 * BLOCK, 256), f32),
        pltpu.VMEM((4, 8, 256), f32),
        pltpu.VMEM((4, 384, 256), f32),
        pltpu.VMEM((4, 8, 256), f32),
        pltpu.VMEM((4, 8, 256), f32),
        *results(4), *results(4), *results(4),
        *results(2, rows=192), *results(2, rows=192), *results(2, rows=192), *results(2, rows=192),
        pltpu.VMEM((384, BLOCK), f32),
        dma((6,)), dma((6,)), dma((4, 2)), dma((4, 2)), dma((5, 2)), dma((5, 2)), dma((4, 2)), dma((4, 2)),
        dma((4,)), dma((4,)), dma((4,)), dma((4,)), dma((6,)), dma((6,)), dma((6,)), dma((6,)),
    ]
    assert len(attention_scratch) == A_COUNT
    return pl.pallas_call(
        layer_kernel,
        out_shape=[jax.ShapeDtypeStruct((BLOCK, 512), bf16)] * 2,
        in_specs=[vmem] * 12 + [hbm] * 10,
        out_specs=[vmem] * 2,
        scratch_shapes=[
            *[pltpu.VMEM(m.shape, bf16) for m in matrices[0:6]],
            pltpu.VMEM((BLOCK, 512), bf16),
            *[pltpu.VMEM(m.shape, bf16) for m in matrices[7:10]],
            pltpu.VMEM((256, 128), bf16), pltpu.VMEM((128, 128), f32), pltpu.VMEM((BLOCK, 384), bf16), dma((10,)),
            *attention_scratch,
            pltpu.VMEM((128, 512), f32),
            half, half, pltpu.VMEM((2, 2, 64, 512), bf16), half, half, half,
            pltpu.VMEM((8, 128), f32), pltpu.VMEM((3, 8, 128), f32),
            chunks(128), chunks(128), chunks(128), chunks(128),
            chunks(512), halves, chunks(512), chunks(512, 4), pltpu.VMEM((256, 512), bf16), chunks(512, 4),
            chunks(512), chunks(512), chunks(512), chunks(512), chunks(512), chunks(512), halves, chunks(512),
            dma((6,)), dma((6,)), dma((3,)), dma((3,)),
            *[dma((8,))] * 4, *[dma((2, 8))] * 2, *[dma((8,))] * 16, *[dma((2, 8))] * 2,
        ],
        compiler_params=pltpu.CompilerParams(
            collective_id=0, has_side_effects=True, vmem_limit_bytes=60 * 1024 * 1024
        ),
        name="layer",
    )(*vectors, *matrices)


def turn_tables(position):
    lane = jnp.arange(128, dtype=jnp.int32)
    frequency = 1.0 / ROPE_BASE ** ((lane % 32).astype(jnp.float32) * 2.0 / ROPE)
    angle = position.astype(jnp.float32)[:, None] * frequency[None, :]
    sign = jnp.where(lane % 64 < 32, -1.0, 1.0)
    return jnp.cos(angle), jnp.sin(angle) * sign[None, :]


def body(
    query_wide,
    query_narrow,
    latent,
    rope_key,
    latent_norm_weight,
    broad_key_lift,
    broad_value_lift,
    slim_key_lift,
    slim_value_lift,
    out_wide,
    out_narrow,
    resid,
    ffn_gain,
    group_route,
    expert_pair,
    group_prob,
    expert_prob,
    gate_weight,
    up_weight,
    down_weight,
):
    cos, sin = turn_tables(lax.axis_index("sp") * BLOCK + jnp.arange(BLOCK, dtype=jnp.int32))
    stream, moe = layer(
        (
            query_wide, query_narrow, latent, rope_key.T, latent_norm_weight[None, :], cos, sin,
            group_route[None, :], expert_pair.T, group_prob[None, :], expert_prob.T, ffn_gain[None, :],
        ),
        (
            broad_key_lift, broad_value_lift, slim_key_lift, slim_value_lift, out_wide, out_narrow, resid,
            gate_weight[0], up_weight[0], down_weight[0],
        ),
    )
    return (stream.astype(jnp.float32) + moe.astype(jnp.float32)).astype(jnp.bfloat16)


def solution(mesh):
    placed = (
        P("sp", "tp"),
        P("sp", "tp"),
        P("sp", None),
        P("sp", None),
        P(),
        P(None, "tp"),
        P(None, "tp"),
        P(None, "tp"),
        P(None, "tp"),
        P("tp", None),
        P("tp", None),
        P("sp", None),
        P(),
        P("sp"),
        P("sp", None),
        P("sp"),
        P("sp", None),
        P("sp", None, None, "tp"),
        P("sp", None, None, "tp"),
        P("sp", None, "tp", None),
    )
    return jax.shard_map(body, mesh=mesh, in_specs=placed, out_specs=P("sp", "tp"), check_vma=False)
```
